32 devices in a mesh: ep: 8 (over z, core), tp: 4 (over y, x).
Axes of the slice: x: 2, y: 2, z: 4, core: 2. Of those that a mesh axis runs over, the one named last changes fastest.
Arguments:
- tokens: bfloat16 [128, 2048], P('ep'), may hold values from -6 to 6
- attn_gain: float32 [2048], replicated, may hold values from 0.1 to 1.9
- query_weight: bfloat16 [2048, 2048], P('ep', 'tp'), may hold values from -0.125 to 0.125
- key_weight: bfloat16 [2048, 2048], P('ep', 'tp'), may hold values from -0.125 to 0.125
- value_weight: bfloat16 [2048, 2048], P('ep', 'tp'), may hold values from -0.125 to 0.125
- forget_weight: bfloat16 [2048, 16], P(None, 'tp'), may hold values from -0.125 to 0.125
- forget_bias: float32 [16], P('tp'), may hold values from -1 to 2
- cache_keys: bfloat16 [128, 16, 384, 128], P('ep', 'tp'), may hold values from -240 to 240
- cache_values: bfloat16 [128, 16, 384, 128], P('ep', 'tp'), may hold values from -6 to 6
- cache_gates: float32 [128, 16, 384], P('ep', 'tp'), may hold values from -768 to 0, as said below
- lengths: int32 [128], P('ep'), may hold values from 1 to 384
- output_weight: bfloat16 [2048, 2048], P('tp', 'ep'), may hold values from -0.125 to 0.125
- ffn_gain: float32 [2048], replicated, may hold values from 0.1 to 1.9
- dense_gate_proj: bfloat16 [2048, 2048], P('ep', 'tp'), may hold values from -0.125 to 0.125
- dense_up_proj: bfloat16 [2048, 2048], P('ep', 'tp'), may hold values from -0.125 to 0.125
- dense_down_proj: bfloat16 [2048, 2048], P('tp', 'ep'), may hold values from -0.125 to 0.125
- dense_mix: bfloat16 [2048], replicated, may hold values from -0.125 to 0.125
- expert_ids: int32 [128, 2], P('ep'), may hold values from 0 to 7, as said below
- group_prob: float32 [128], P('ep'), may hold values from 0.25 to 1
- pair_prob: float32 [128, 2], P('ep'), may hold values from 0.05 to 1
- expert_gate: bfloat16 [8, 2048, 2048], P('ep', None, 'tp'), may hold values from -0.125 to 0.125
- expert_up: bfloat16 [8, 2048, 2048], P('ep', None, 'tp'), may hold values from -0.125 to 0.125
- expert_down: bfloat16 [8, 2048, 2048], P('ep', 'tp'), may hold values from -0.125 to 0.125
Outputs:
- mixed_out: bfloat16 [128, 2048], P('ep')
The draws below stay inside these ranges and needn't reach their ends.
Inputs may be any that keep to these rules, and one draw needn't show every extreme that they name: `expert_ids`: each row names two different experts of one group, the groups being 4 runs of consecutive ids. In each aligned block of 16 rows (the rows of one index of ep) no expert is named more than 8 times, and some expert exactly 8 times. `cache_gates`: along positions the values never rise.
All inputs are finite; a program needn't handle non-finite values.
Results may differ from the reference program's by a relative error of at most 0.014.
Values may be sent and summed in bfloat16 or wider, within the bound.
A program may use at most 64 MiB of HBM per device.

```python
import math
import jax
import jax.numpy as jnp
from jax import lax

D = 2048
HEAD_TOTAL = 16
HEAD = 128
FF_D = 2048
FF_E = 2048
GROUPS = 4
SEQ_DEV = 16
CACHED_LENGTH = 384
SEQUENCE_TOTAL = 128
EXPERTS = 8
CAP = 8
N_EP = 8


def draw_cache_keys(key, part):
    first_key = jax.random.fold_in(key, 0)
    base = jnp.clip(jax.random.normal(first_key, (SEQUENCE_TOTAL, HEAD_TOTAL, CACHED_LENGTH, HEAD), jnp.float32), -6.0, 6.0)
    return base.astype(jnp.bfloat16)


def draw_cache_gates(key, part):
    every_key = jax.random.split(key, 7)
    fast_share = 0.5
    fast_heads = jax.random.uniform(every_key[0], (1, HEAD_TOTAL, 1), jnp.float32) < fast_share
    slow_rate = jnp.exp(jax.random.uniform(every_key[1], (SEQUENCE_TOTAL, HEAD_TOTAL, 1), jnp.float32, math.log(0.3), math.log(2.0))) / CACHED_LENGTH
    fast_rate = jnp.exp(jax.random.uniform(every_key[2], (SEQUENCE_TOTAL, HEAD_TOTAL, 1), jnp.float32, math.log(1.0 / 100.0), math.log(1.0 / 30.0)))
    seq_factor = jnp.exp(jax.random.uniform(every_key[3], (SEQUENCE_TOTAL, 1, 1), jnp.float32, math.log(0.5), math.log(2.0)))
    coarse_scores = jax.random.uniform(every_key[4], (SEQUENCE_TOTAL, HEAD_TOTAL, CACHED_LENGTH), jnp.float32, 0.3, 1.7)
    decay_rate = jnp.where(fast_heads, fast_rate, slow_rate) * seq_factor
    spike_mask = jax.random.uniform(every_key[5], (SEQUENCE_TOTAL, HEAD_TOTAL, CACHED_LENGTH), jnp.float32) < 3.0 / CACHED_LENGTH
    spike_length = jnp.log(jax.random.uniform(every_key[6], (SEQUENCE_TOTAL, HEAD_TOTAL, CACHED_LENGTH), jnp.float32, 0.5, 0.8))
    gate_logs = -decay_rate * coarse_scores + jnp.where(spike_mask, spike_length, 0.0)
    return jnp.cumsum(gate_logs, axis=-1).astype(jnp.float32)


def draw_expert_ids(key, part):
    group_width = EXPERTS // GROUPS
    pair_count = CAP * group_width // 2

    def one_block(block_key):
        every_key = jax.random.split(block_key, 4)
        heavy = jax.random.randint(every_key[0], (), 0, GROUPS)
        perm_keys = jax.random.split(every_key[1], GROUPS * CAP)
        orders = jax.vmap(lambda perm_key: jax.random.permutation(perm_key, group_width))(perm_keys)
        orders = orders.reshape(GROUPS, CAP * group_width).astype(jnp.int32)
        orders = orders + (jnp.arange(GROUPS, dtype=jnp.int32) * group_width)[:, None]
        pair_ids = orders.reshape(GROUPS * pair_count, 2)
        ranking = jax.random.permutation(every_key[2], GROUPS * pair_count).astype(jnp.int32)
        group_of = jnp.arange(GROUPS * pair_count, dtype=jnp.int32) // pair_count
        priority = jnp.where(group_of == heavy, 0, GROUPS * pair_count) + ranking
        chosen = jnp.argsort(priority, stable=True)[:SEQ_DEV]
        picked = pair_ids[chosen]
        shuffle = jax.random.permutation(every_key[3], SEQ_DEV)
        return picked[shuffle]
    block_keys = jax.random.split(key, SEQUENCE_TOTAL // SEQ_DEV)
    return jax.vmap(one_block)(block_keys).reshape(SEQUENCE_TOTAL, 2).astype(jnp.int32)


def with_ends(values, key, smallest, high):
    spot = [jax.random.randint(jax.random.fold_in(key, axis), (), 0, length) for axis, length in enumerate(values.shape)]
    main_axis = values.shape.index(max(values.shape))
    beside = spot[:main_axis] + [(spot[main_axis] + 1) % values.shape[main_axis]] + spot[main_axis + 1:]
    return values.at[tuple(spot)].set(smallest).at[tuple(beside)].set(high)


def shard_levels(key, shape, shards, low, high):
    factor_of = 1.0
    for axis_at, parts in shards:
        draws = jax.random.uniform(jax.random.fold_in(jax.random.fold_in(key, 6), axis_at), (parts,), jnp.float32, low / len(shards), high / len(shards))
        factor_of = factor_of * jnp.repeat(jnp.exp(draws), shape[axis_at] // parts).reshape((-1,) + (1,) * (len(shape) - 1 - axis_at))
    return factor_of


def gaussian(key, dims, scale, bound, shards=(), held_as=jnp.bfloat16):
    array = scale * jax.random.normal(key, dims, jnp.float32)
    if shards:
        array = array * shard_levels(key, dims, shards, -0.22, 0.18)
    return jnp.clip(array, -bound, bound).astype(held_as)


def setup_inputs(seed: int = 0) -> dict:
    seeds = jax.random.split(jax.random.key(seed), 24)
    return {
        "tokens": gaussian(seeds[0], (SEQUENCE_TOTAL, D), 1.0, 6.0, ((0, 8),)),
        "attn_gain": jnp.clip(1.0 + 0.18 * jax.random.normal(seeds[1], (D,), jnp.float32), 0.1, 1.9),
        "query_weight": gaussian(seeds[2], (D, HEAD_TOTAL * HEAD), D ** -0.5, 0.125, ((0, 8), (1, 4))),
        "key_weight": gaussian(seeds[3], (D, HEAD_TOTAL * HEAD), D ** -0.5, 0.125, ((0, 8), (1, 4))),
        "value_weight": gaussian(seeds[4], (D, HEAD_TOTAL * HEAD), D ** -0.5, 0.125, ((0, 8), (1, 4))),
        "forget_weight": gaussian(seeds[5], (D, HEAD_TOTAL), D ** -0.5, 0.125, ((1, 4),)),
        "forget_bias": jnp.clip(-1.0 + 3.0 * jax.random.uniform(seeds[6], (HEAD_TOTAL,), jnp.float32) ** shard_levels(seeds[6], (HEAD_TOTAL,), ((0, 4),), -0.2, 0.2), -1.0, 2.0),
        "cache_keys": draw_cache_keys(jax.random.fold_in(seeds[23], 71), 0),
        "cache_values": gaussian(seeds[8], (SEQUENCE_TOTAL, HEAD_TOTAL, CACHED_LENGTH, HEAD), 1.0, 6.0, ((0, 8), (1, 4))),
        "cache_gates": draw_cache_gates(jax.random.fold_in(seeds[23], 71), 0),
        "lengths": with_ends(jax.random.randint(seeds[10], (SEQUENCE_TOTAL,), 1, CACHED_LENGTH + 1), jax.random.fold_in(seeds[10], 1), 1, CACHED_LENGTH).astype(jnp.int32),
        "output_weight": gaussian(seeds[11], (HEAD_TOTAL * HEAD, D), (HEAD_TOTAL * HEAD) ** -0.5, 0.125, ((0, 4), (1, 8))),
        "ffn_gain": jnp.clip(1.0 + 0.18 * jax.random.normal(seeds[12], (D,), jnp.float32), 0.1, 1.9),
        "dense_gate_proj": gaussian(seeds[13], (D, FF_D), D ** -0.5, 0.125, ((0, 8), (1, 4))),
        "dense_up_proj": gaussian(seeds[14], (D, FF_D), D ** -0.5, 0.125, ((0, 8), (1, 4))),
        "dense_down_proj": gaussian(seeds[15], (FF_D, D), FF_D ** -0.5, 0.125, ((0, 4), (1, 8))),
        "dense_mix": gaussian(seeds[16], (D,), D ** -0.5, 0.125),
        "expert_ids": draw_expert_ids(jax.random.fold_in(seeds[23], 71), 0),
        "group_prob": jnp.clip(jnp.exp(math.log(1.0) - 1.3862944 * jax.random.uniform(seeds[18], (SEQUENCE_TOTAL,), jnp.float32) ** shard_levels(seeds[18], (SEQUENCE_TOTAL,), ((0, 8),), -0.2, 0.2)), 0.25, 1.0),
        "pair_prob": jnp.clip(0.05 + 0.95 * jax.random.uniform(seeds[19], (SEQUENCE_TOTAL, 2), jnp.float32) ** shard_levels(seeds[19], (SEQUENCE_TOTAL, 2), ((0, 8),), -0.2, 0.2), 0.05, 1.0),
        "expert_gate": gaussian(seeds[20], (EXPERTS, D, FF_E), D ** -0.5, 0.125, ((0, 8), (2, 4))),
        "expert_up": gaussian(seeds[21], (EXPERTS, D, FF_E), D ** -0.5, 0.125, ((0, 8), (2, 4))),
        "expert_down": gaussian(seeds[22], (EXPERTS, FF_E, D), FF_E ** -0.5, 0.125, ((0, 8), (1, 4))),
    }


EPSILON = 1e-06

def rms_scale(values, norm_gain):
    widened = values.astype(jnp.float32)
    return widened * lax.rsqrt(lax.optimization_barrier(jnp.mean(widened * widened, axis=-1, keepdims=True)) + EPSILON) * norm_gain

def attend(members):
    queries, keys_new, values_new, key_cache, value_cache, gate_cache, lengths, log_forget = members
    cache_span = key_cache.shape[2]
    score_scale = 1.0 / math.sqrt(key_cache.shape[3])
    positions = jnp.arange(cache_span, dtype=jnp.int32)
    live_mask = positions[None, :] < lengths[:, None]
    last_mask = positions[None, :] == lengths[:, None] - 1
    last_gate = lax.optimization_barrier(jnp.sum(jnp.where(last_mask[:, None, :], gate_cache, 0.0), axis=-1))
    gate_now = last_gate + log_forget
    scores = jnp.einsum('shd,shpd->shp', queries.astype(jnp.float32), key_cache.astype(jnp.float32)) * score_scale
    scores = scores + gate_now[:, :, None] - gate_cache
    scores = jnp.where(live_mask[:, None, :], scores, -jnp.inf)
    own_score = lax.optimization_barrier(jnp.sum(queries.astype(jnp.float32) * keys_new.astype(jnp.float32), axis=-1)) * score_scale
    row_top = jnp.maximum(lax.optimization_barrier(jnp.max(scores, axis=-1)), own_score)
    raised = jnp.exp(scores - row_top[:, :, None])
    own_raised = jnp.exp(own_score - row_top)
    totals = lax.optimization_barrier(jnp.sum(raised, axis=-1)) + own_raised
    weights_low = (raised / totals[:, :, None]).astype(jnp.bfloat16)
    own_prob = (own_raised / totals).astype(jnp.bfloat16)
    attended = jnp.einsum('shp,shpd->shd', weights_low.astype(jnp.float32), value_cache.astype(jnp.float32))
    attended = attended + own_prob.astype(jnp.float32)[:, :, None] * values_new.astype(jnp.float32)
    return attended.astype(jnp.bfloat16)

def by_block(array_in):
    return array_in.reshape((N_EP, array_in.shape[0] // N_EP) + array_in.shape[1:])

def reference(tokens, attn_gain, query_weight, key_weight, value_weight, forget_weight, forget_bias, cache_keys, cache_values, cache_gates, lengths, output_weight, ffn_gain, dense_gate_proj, dense_up_proj, dense_down_proj, dense_mix, expert_ids, group_prob, pair_prob, expert_gate, expert_up, expert_down):
    seq_count = tokens.shape[0]
    normed = rms_scale(tokens, attn_gain).astype(jnp.bfloat16)
    queries = jnp.dot(normed, query_weight, preferred_element_type=jnp.float32).astype(jnp.bfloat16)
    keys_new = jnp.dot(normed, key_weight, preferred_element_type=jnp.float32).astype(jnp.bfloat16)
    values_new = jnp.dot(normed, value_weight, preferred_element_type=jnp.float32).astype(jnp.bfloat16)
    queries = queries.reshape(seq_count, HEAD_TOTAL, HEAD)
    keys_new = keys_new.reshape(seq_count, HEAD_TOTAL, HEAD)
    values_new = values_new.reshape(seq_count, HEAD_TOTAL, HEAD)
    log_forget = jax.nn.log_sigmoid(jnp.dot(normed, forget_weight, preferred_element_type=jnp.float32) + forget_bias)
    members = tuple((by_block(item) for item in (queries, keys_new, values_new, cache_keys, cache_values, cache_gates, lengths, log_forget)))
    attended = lax.map(attend, members).reshape(seq_count, HEAD_TOTAL * HEAD)
    residual = (tokens.astype(jnp.float32) + jnp.dot(attended, output_weight, preferred_element_type=jnp.float32)).astype(jnp.bfloat16)
    ffn_in = rms_scale(residual, ffn_gain).astype(jnp.bfloat16)
    dense_gate_part = jnp.dot(ffn_in, dense_gate_proj, preferred_element_type=jnp.float32)
    dense_up_part = jnp.dot(ffn_in, dense_up_proj, preferred_element_type=jnp.float32)
    dense_hidden = (jax.nn.silu(dense_gate_part) * dense_up_part).astype(jnp.bfloat16)
    dense_total = jnp.dot(dense_hidden, dense_down_proj, preferred_element_type=jnp.float32)
    mix = jax.nn.sigmoid(jnp.dot(ffn_in, dense_mix, preferred_element_type=jnp.float32))
    routes = group_prob[:, None] * pair_prob / lax.optimization_barrier(jnp.sum(pair_prob, axis=1, keepdims=True))
    most_rows = CAP * N_EP

    def one_expert(accum, expert_index):
        hit_mask = expert_ids == expert_index
        row_weight = lax.optimization_barrier(jnp.sum(jnp.where(hit_mask, routes, 0.0), axis=1))
        any_hit = lax.optimization_barrier(jnp.sum(hit_mask.astype(jnp.int32), axis=1)) > 0
        chosen = jnp.nonzero(any_hit, size=most_rows, fill_value=0)[0].astype(jnp.int32)
        valid_rows = jnp.arange(most_rows, dtype=jnp.int32) < jnp.sum(any_hit.astype(jnp.int32))
        row_data = ffn_in[chosen]
        gate_part = jnp.dot(row_data, expert_gate[expert_index], preferred_element_type=jnp.float32)
        up_part = jnp.dot(row_data, expert_up[expert_index], preferred_element_type=jnp.float32)
        expert_hidden = (jax.nn.silu(gate_part) * up_part).astype(jnp.bfloat16)
        expert_out = jnp.dot(expert_hidden, expert_down[expert_index], preferred_element_type=jnp.float32)
        weight_rows = jnp.where(valid_rows, row_weight[chosen], 0.0)
        return (accum.at[chosen].add(weight_rows[:, None] * expert_out), None)
    expert_sum, _ = lax.scan(one_expert, jnp.zeros((seq_count, D), jnp.float32), jnp.arange(EXPERTS, dtype=jnp.int32))
    result = residual.astype(jnp.float32) + expert_sum + mix[:, None] * dense_total
    return result.astype(jnp.bfloat16)
```

```python
import functools
import math

import jax
import jax.numpy as jnp
from jax import lax
from jax.experimental import pallas as pl
from jax.experimental.pallas import tpu as pltpu
from jax.sharding import PartitionSpec as P

EPSILON = 1e-06


def rms_scale(values, norm_gain):
    widened = values.astype(jnp.float32)
    return (
        widened
        * lax.rsqrt(jnp.mean(widened * widened, axis=-1, keepdims=True) + EPSILON)
        * norm_gain
    )


def attend(queries, keys_new, values_new, key_cache, value_cache, gate_cache, lengths, log_forget):
    cache_span = key_cache.shape[2]
    score_scale = 1.0 / math.sqrt(key_cache.shape[3])
    positions = jnp.arange(cache_span, dtype=jnp.int32)
    live_mask = positions[None, :] < lengths[:, None]
    last_mask = positions[None, :] == lengths[:, None] - 1
    last_gate = jnp.sum(jnp.where(last_mask[:, None, :], gate_cache, 0.0), axis=-1)
    gate_now = last_gate + log_forget
    scores = (
        jnp.einsum("shd,shpd->shp", queries, key_cache, preferred_element_type=jnp.float32)
        * score_scale
    )
    scores = scores + gate_now[:, :, None] - gate_cache
    scores = jnp.where(live_mask[:, None, :], scores, -jnp.inf)
    own_score = (
        jnp.sum(queries.astype(jnp.float32) * keys_new.astype(jnp.float32), axis=-1) * score_scale
    )
    row_top = jnp.maximum(jnp.max(scores, axis=-1), own_score)
    raised = jnp.exp(scores - row_top[:, :, None])
    own_raised = jnp.exp(own_score - row_top)
    totals = jnp.sum(raised, axis=-1) + own_raised
    weights_low = (raised / totals[:, :, None]).astype(jnp.bfloat16)
    own_prob = (own_raised / totals).astype(jnp.bfloat16)
    attended = jnp.einsum(
        "shp,shpd->shd", weights_low, value_cache, preferred_element_type=jnp.float32
    )
    attended = attended + own_prob.astype(jnp.float32)[:, :, None] * values_new.astype(jnp.float32)
    return attended.astype(jnp.bfloat16)


MESH = pl.DeviceIdType.MESH
F32 = jnp.float32
BF16 = jnp.bfloat16


def fan_out(axis, count, me, source_of, landing, send_sem, recv_sem):
    copies = []
    for step in range(1, count):
        target = lax.rem(me + step, count)
        copy = pltpu.make_async_remote_copy(
            src_ref=source_of(target),
            dst_ref=landing.at[me],
            send_sem=send_sem.at[step],
            recv_sem=recv_sem.at[me],
            device_id={axis: target},
            device_id_type=MESH,
        )
        copy.start()
        copies.append(copy)
    return copies


def collect(axis, count, me, landing, send_sem, recv_sem):
    for step in range(1, count):
        source = lax.rem(me + count - step, count)
        pltpu.make_async_remote_copy(
            src_ref=landing.at[source],
            dst_ref=landing.at[source],
            send_sem=send_sem.at[step],
            recv_sem=recv_sem.at[source],
            device_id={axis: source},
            device_id_type=MESH,
        ).wait_recv()


def spread_rows(axis_ep, axis_tp, n_ep, n_tp, me_ep, me_tp, held, landing, send_sem, recv_sem):
    ratio = n_ep // n_tp
    for part in range(ratio):
        target_ep = me_tp * ratio + part
        for step in range(n_tp):
            target_tp = lax.rem(me_tp + step, n_tp)

            def send():
                pltpu.make_async_remote_copy(
                    src_ref=held.at[part],
                    dst_ref=landing.at[me_ep],
                    send_sem=send_sem.at[part * n_tp + step],
                    recv_sem=recv_sem.at[me_ep],
                    device_id={axis_ep: target_ep, axis_tp: target_tp},
                    device_id_type=MESH,
                ).start()

            if step == 0:
                pl.when(target_ep != me_ep)(send)

                @pl.when(target_ep == me_ep)
                def _():
                    landing[me_ep] = held[part]
            else:
                send()


def spread_wait(axis_ep, axis_tp, n_ep, n_tp, me_ep, me_tp, held, landing, send_sem, recv_sem):
    ratio = n_ep // n_tp
    own_tp = me_ep // ratio
    for step in range(n_ep):
        source = lax.rem(me_ep + n_ep - step, n_ep)

        def arrive():
            pltpu.make_async_remote_copy(
                src_ref=landing.at[source],
                dst_ref=landing.at[source],
                send_sem=send_sem.at[0],
                recv_sem=recv_sem.at[source],
                device_id={axis_ep: source, axis_tp: own_tp},
                device_id_type=MESH,
            ).wait_recv()

        if step == 0:
            pl.when(own_tp != me_tp)(arrive)
        else:
            arrive()


def spread_sent(axis_ep, axis_tp, n_ep, n_tp, me_ep, me_tp, held, landing, send_sem, recv_sem):
    ratio = n_ep // n_tp
    for part in range(ratio):
        target_ep = me_tp * ratio + part
        for step in range(n_tp):
            target_tp = lax.rem(me_tp + step, n_tp)

            def sent():
                pltpu.make_async_remote_copy(
                    src_ref=held.at[part],
                    dst_ref=landing.at[me_ep],
                    send_sem=send_sem.at[part * n_tp + step],
                    recv_sem=recv_sem.at[me_ep],
                    device_id={axis_ep: target_ep, axis_tp: target_tp},
                    device_id_type=MESH,
                ).wait_send()

            if step == 0:
                pl.when(target_ep != me_ep)(sent)
            else:
                sent()


def total_of(ref, count):
    total = ref[0].astype(F32)
    for index in range(1, count):
        total = total + ref[index].astype(F32)
    return total


def dot32(left, right):
    return jnp.dot(left, right, preferred_element_type=F32)


def project_kernel(
    n_ep,
    tokens,
    gain,
    query_weight,
    key_weight,
    value_weight,
    queries,
    keys_new,
    values_new,
    normed_out,
    norm_send,
    norm_land,
    part_send,
    part_land,
    norm_ss,
    norm_rs,
    part_ss,
    part_rs,
):
    me = lax.axis_index("ep")
    barrier = pltpu.get_barrier_semaphore()
    for step in range(1, n_ep):
        pl.semaphore_signal(
            barrier, inc=1, device_id={"ep": lax.rem(me + step, n_ep)}, device_id_type=MESH
        )
    rows, depth = norm_send.shape[1:]
    width = query_weight.shape[1]
    normed = rms_scale(tokens[...], gain[...])
    normed_out[...] = normed.astype(BF16)
    for index in range(n_ep):
        norm_send[index] = normed[:, index * depth : (index + 1) * depth].astype(BF16)
    pl.semaphore_wait(barrier, n_ep - 1)
    sent = fan_out("ep", n_ep, me, lambda t: norm_send.at[t], norm_land, norm_ss, norm_rs)
    norm_land[me] = norm_send[me]
    collect("ep", n_ep, me, norm_land, norm_ss, norm_rs)
    joined = norm_land[...].reshape(n_ep * rows, depth)
    for index, weight in enumerate((query_weight, key_weight, value_weight)):
        part_send[:, :, index * width : (index + 1) * width] = dot32(joined, weight[...]).reshape(
            n_ep, rows, width
        )
    sent += fan_out("ep", n_ep, me, lambda t: part_send.at[t], part_land, part_ss, part_rs)
    part_land[me] = part_send[me]
    collect("ep", n_ep, me, part_land, part_ss, part_rs)
    total = total_of(part_land, n_ep).astype(BF16)
    queries[...] = total[:, :width]
    keys_new[...] = total[:, width : 2 * width]
    values_new[...] = total[:, 2 * width :]
    for copy in sent:
        copy.wait_send()


def project(n_ep, tokens, gain, query_weight, key_weight, value_weight):
    rows, model = tokens.shape
    depth, width = query_weight.shape
    vmem = pl.BlockSpec(memory_space=pltpu.VMEM)
    sems = pltpu.SemaphoreType.DMA((n_ep,))
    head_shape = jax.ShapeDtypeStruct((rows, width), BF16)
    return pl.pallas_call(
        functools.partial(project_kernel, n_ep),
        out_shape=(head_shape,) * 3 + (jax.ShapeDtypeStruct((rows, model), BF16),),
        in_specs=[vmem] * 5,
        out_specs=(vmem,) * 4,
        scratch_shapes=[
            pltpu.VMEM((n_ep, rows, depth), BF16),
            pltpu.VMEM((n_ep, rows, depth), BF16),
            pltpu.VMEM((n_ep, rows, 3 * width), F32),
            pltpu.VMEM((n_ep, rows, 3 * width), F32),
            sems,
            sems,
            sems,
            sems,
        ],
        compiler_params=pltpu.CompilerParams(collective_id=0, has_side_effects=True),
    )(tokens, gain.reshape(1, model), query_weight, key_weight, value_weight)


def feed_kernel(
    n_ep,
    n_tp,
    attended,
    tokens,
    gain,
    output_weight,
    dense_gate,
    dense_up,
    dense_down,
    dense_mix,
    to_slots,
    from_first,
    from_second,
    routes,
    expert_gate,
    expert_up,
    expert_down,
    out,
    gate_held,
    up_held,
    down_held,
    full,
    att_land,
    head_send,
    head_land,
    mix_send,
    mix_land,
    ffn_send,
    ffn_land,
    slot_send,
    slot_land,
    dense_send,
    dense_land,
    expert_send,
    expert_land,
    back_send,
    back_land,
    hidden_send,
    hidden_land,
    down_send,
    down_land,
    tail_send,
    tail_land,
    route_send,
    route_land,
    load_sem,
    att_ss,
    att_rs,
    head_ss,
    head_rs,
    mix_ss,
    mix_rs,
    ffn_ss,
    ffn_rs,
    slot_ss,
    slot_rs,
    dense_ss,
    dense_rs,
    expert_ss,
    expert_rs,
    back_ss,
    back_rs,
    hidden_ss,
    hidden_rs,
    down_ss,
    down_rs,
    tail_ss,
    tail_rs,
    route_ss,
    route_rs,
):
    me = lax.axis_index("ep")
    me_tp = lax.axis_index("tp")
    barrier = pltpu.get_barrier_semaphore()
    everyone = n_ep * n_tp
    place = me * n_tp + me_tp

    def greet(step, carry):
        other = lax.rem(place + step, everyone)
        pl.semaphore_signal(
            barrier,
            inc=1,
            device_id={"ep": other // n_tp, "tp": lax.rem(other, n_tp)},
            device_id_type=MESH,
        )
        return carry

    lax.fori_loop(1, everyone, greet, 0)
    loads = [
        pltpu.make_async_copy(expert_gate, gate_held, load_sem.at[0]),
        pltpu.make_async_copy(expert_up, up_held, load_sem.at[1]),
        pltpu.make_async_copy(expert_down, down_held, load_sem.at[2]),
    ]
    for load in loads:
        load.start()
    pl.semaphore_wait(barrier, everyone - 1)

    rows, model = tokens.shape
    hidden = dense_gate.shape[1]
    depth = dense_gate.shape[0]
    slots = slot_send.shape[1]
    group_rows = n_ep * rows // n_tp
    ratio = n_ep // n_tp
    grid = (n_ep, n_tp, me, me_tp)

    sent = fan_out("ep", n_ep, me, lambda t: attended, att_land, att_ss, att_rs)
    att_land[me] = attended[...]
    collect("ep", n_ep, me, att_land, att_ss, att_rs)
    shares = dot32(att_land[...].reshape(n_ep * rows, hidden), output_weight[...])
    head_send[...] = shares.reshape(n_tp, group_rows, depth)
    sent += fan_out("tp", n_tp, me_tp, lambda t: head_send.at[t], head_land, head_ss, head_rs)
    head_land[me_tp] = head_send[me_tp]
    collect("tp", n_tp, me_tp, head_land, head_ss, head_rs)
    mix_send[...] = total_of(head_land, n_tp).reshape(ratio, rows, depth)
    spread_rows("ep", "tp", *grid, mix_send, mix_land, mix_ss, mix_rs)
    spread_wait("ep", "tp", *grid, mix_send, mix_land, mix_ss, mix_rs)
    for index in range(n_ep):
        full[:, index * depth : (index + 1) * depth] = mix_land[index]
    residual = (tokens[...].astype(F32) + full[...]).astype(BF16)
    ffn_wide = rms_scale(residual, gain[...])
    ffn_in = ffn_wide.astype(BF16)

    for index in range(n_ep):
        ffn_send[index] = ffn_wide[:, index * depth : (index + 1) * depth].astype(BF16)
    sent += fan_out("ep", n_ep, me, lambda t: ffn_send.at[t], ffn_land, ffn_ss, ffn_rs)
    outbound = dot32(to_slots[...], ffn_in)
    for index in range(n_ep):
        slot_send[index] = outbound[index * slots : (index + 1) * slots].astype(BF16)
    sent += fan_out("ep", n_ep, me, lambda t: slot_send.at[t], slot_land, slot_ss, slot_rs)
    ffn_land[me] = ffn_send[me]
    slot_land[me] = slot_send[me]
    mix = jax.nn.sigmoid(
        jnp.sum(ffn_in.astype(F32) * dense_mix[...].astype(F32), axis=-1, keepdims=True)
    )

    collect("ep", n_ep, me, ffn_land, ffn_ss, ffn_rs)
    ffn_rows = ffn_land[...].reshape(n_ep * rows, depth)
    for index, weight in enumerate((dense_gate, dense_up)):
        dense_send[:, :, index * hidden : (index + 1) * hidden] = (
            dot32(ffn_rows, weight[...]).astype(BF16).reshape(n_ep, rows, hidden)
        )
    sent += fan_out("ep", n_ep, me, lambda t: dense_send.at[t], dense_land, dense_ss, dense_rs)
    dense_land[me] = dense_send[me]

    collect("ep", n_ep, me, slot_land, slot_ss, slot_rs)
    for load in loads:
        load.wait()
    slot_rows = jnp.concatenate(
        [slot_land[index].astype(F32) for index in range(n_ep)], axis=0
    ).astype(BF16)
    gate_part = dot32(slot_rows, gate_held[0])
    up_part = dot32(slot_rows, up_held[0])
    expert_hidden = (gate_part / (1.0 + jnp.exp(-gate_part)) * up_part).astype(BF16)
    chunk = model // n_tp
    for index in range(n_tp):
        expert_send[index] = dot32(
            expert_hidden, down_held[0, :, index * chunk : (index + 1) * chunk]
        ).astype(BF16)
    sent += fan_out(
        "tp", n_tp, me_tp, lambda t: expert_send.at[t], expert_land, expert_ss, expert_rs
    )
    expert_land[me_tp] = expert_send[me_tp]

    collect("ep", n_ep, me, dense_land, dense_ss, dense_rs)
    dense_sum = total_of(dense_land, n_ep)
    dense_first = dense_sum[:, :hidden]
    hidden_send[...] = (
        dense_first / (1.0 + jnp.exp(-dense_first)) * dense_sum[:, hidden:]
    ).astype(BF16)
    sent += fan_out("ep", n_ep, me, lambda t: hidden_send, hidden_land, hidden_ss, hidden_rs)
    hidden_land[me] = hidden_send[...]

    collect("tp", n_tp, me_tp, expert_land, expert_ss, expert_rs)
    expert_total = total_of(expert_land, n_tp)
    for index in range(n_ep):
        back_send[index] = expert_total[index * slots : (index + 1) * slots].astype(BF16)
    sent += fan_out("ep", n_ep, me, lambda t: back_send.at[t], back_land, back_ss, back_rs)
    back_land[me] = back_send[me]

    collect("ep", n_ep, me, hidden_land, hidden_ss, hidden_rs)
    down = dot32(hidden_land[...].reshape(n_ep * rows, hidden), dense_down[...])
    down_send[...] = down.astype(BF16).reshape(n_tp, group_rows, depth)
    sent += fan_out("tp", n_tp, me_tp, lambda t: down_send.at[t], down_land, down_ss, down_rs)
    down_land[me_tp] = down_send[me_tp]

    collect("ep", n_ep, me, back_land, back_ss, back_rs)
    back_rows = jnp.concatenate(
        [back_land[index].astype(F32) for index in range(n_ep)], axis=0
    ).astype(BF16)
    route_send[...] = routes[:, 0:1] * dot32(from_first[...], back_rows) + routes[:, 1:2] * dot32(
        from_second[...], back_rows
    )
    sent += fan_out("tp", n_tp, me_tp, lambda t: route_send, route_land, route_ss, route_rs)
    route_land[me_tp] = route_send[...]

    collect("tp", n_tp, me_tp, down_land, down_ss, down_rs)
    tail_send[...] = total_of(down_land, n_tp).astype(BF16).reshape(ratio, rows, depth)
    spread_rows("ep", "tp", *grid, tail_send, tail_land, tail_ss, tail_rs)
    collect("tp", n_tp, me_tp, route_land, route_ss, route_rs)
    spread_wait("ep", "tp", *grid, tail_send, tail_land, tail_ss, tail_rs)
    for index in range(n_ep):
        full[:, index * depth : (index + 1) * depth] = tail_land[index].astype(F32)
    for index in range(n_tp):
        span = slice(index * chunk, (index + 1) * chunk)
        out[:, span] = (
            residual[:, span].astype(F32) + route_land[index] + mix * full[:, span]
        ).astype(BF16)
    for copy in sent:
        copy.wait_send()
    spread_sent("ep", "tp", *grid, mix_send, mix_land, mix_ss, mix_rs)
    spread_sent("ep", "tp", *grid, tail_send, tail_land, tail_ss, tail_rs)


def feed(n_ep, n_tp, slots, attended, tokens, gain, weights, mix, selectors, routes, experts):
    rows, model = tokens.shape
    depth, hidden = weights[1].shape
    group_rows = n_ep * rows // n_tp
    ratio = n_ep // n_tp
    chunk = model // n_tp
    vmem = pl.BlockSpec(memory_space=pltpu.VMEM)
    hbm = pl.BlockSpec(memory_space=pl.ANY)

    def sems(count):
        return [pltpu.SemaphoreType.DMA((count,))] * 2

    def pair(shape, dtype):
        return [pltpu.VMEM(shape, dtype)] * 2

    return pl.pallas_call(
        functools.partial(feed_kernel, n_ep, n_tp),
        out_shape=jax.ShapeDtypeStruct((rows, model), BF16),
        in_specs=[vmem] * 12 + [hbm] * 3,
        out_specs=vmem,
        scratch_shapes=[pltpu.VMEM(item.shape, item.dtype) for item in experts]
        + [pltpu.VMEM((rows, model), F32), pltpu.VMEM((n_ep, rows, hidden), BF16)]
        + pair((n_tp, group_rows, depth), F32)
        + [pltpu.VMEM((ratio, rows, depth), F32), pltpu.VMEM((n_ep, rows, depth), F32)]
        + pair((n_ep, rows, depth), BF16)
        + pair((n_ep, slots, model), BF16)
        + pair((n_ep, rows, 2 * hidden), BF16)
        + pair((n_tp, n_ep * slots, chunk), BF16)
        + pair((n_ep, slots, chunk), BF16)
        + [pltpu.VMEM((rows, hidden), BF16), pltpu.VMEM((n_ep, rows, hidden), BF16)]
        + pair((n_tp, group_rows, depth), BF16)
        + [pltpu.VMEM((ratio, rows, depth), BF16), pltpu.VMEM((n_ep, rows, depth), BF16)]
        + [pltpu.VMEM((rows, chunk), F32), pltpu.VMEM((n_tp, rows, chunk), F32)]
        + [pltpu.SemaphoreType.DMA((3,))]
        + sems(n_ep)
        + sems(n_tp)
        + sems(n_ep)
        + sems(n_ep)
        + sems(n_ep)
        + sems(n_ep)
        + sems(n_tp)
        + sems(n_ep)
        + sems(n_ep)
        + sems(n_tp)
        + sems(n_ep)
        + sems(n_tp),
        compiler_params=pltpu.CompilerParams(
            collective_id=1, has_side_effects=True, vmem_limit_bytes=40 * 1024 * 1024
        ),
    )(attended, tokens, gain.reshape(1, model), *weights, mix.reshape(1, model), *selectors, routes, *experts)


def shards(
    tokens,
    attn_gain,
    query_weight,
    key_weight,
    value_weight,
    forget_weight,
    forget_bias,
    cache_keys,
    cache_values,
    cache_gates,
    lengths,
    output_weight,
    ffn_gain,
    dense_gate_proj,
    dense_up_proj,
    dense_down_proj,
    dense_mix,
    expert_ids,
    group_prob,
    pair_prob,
    expert_gate,
    expert_up,
    expert_down,
):
    seq_count = tokens.shape[0]
    head_count = cache_keys.shape[1]
    head_size = cache_keys.shape[3]
    n_ep = lax.axis_size("ep")
    n_tp = lax.axis_size("tp")
    queries, keys_new, values_new, normed = project(
        n_ep, tokens, attn_gain, query_weight, key_weight, value_weight
    )
    heads = (seq_count, head_count, head_size)
    log_forget = jax.nn.log_sigmoid(
        jnp.dot(normed, forget_weight, preferred_element_type=jnp.float32) + forget_bias
    )
    attended = attend(
        queries.reshape(heads),
        keys_new.reshape(heads),
        values_new.reshape(heads),
        cache_keys,
        cache_values,
        cache_gates,
        lengths,
        log_forget,
    ).reshape(seq_count, head_count * head_size)

    expert_count = n_ep * expert_gate.shape[0]
    capacity = max(4 * seq_count // expert_count, 8)
    slot_total = expert_count * capacity
    picks = expert_ids.reshape(-1)
    same = (picks[:, None] == picks[None, :]).astype(jnp.int32)
    before = jnp.tril(jnp.ones((2 * seq_count, 2 * seq_count), jnp.int32), -1)
    slot_rank = jnp.sum(same * before, axis=1)
    destination = (picks * capacity + slot_rank).reshape(seq_count, 2)
    slot_grid = jnp.arange(slot_total, dtype=jnp.int32)
    select_first = (destination[:, 0:1] == slot_grid[None, :]).astype(jnp.bfloat16)
    select_second = (destination[:, 1:2] == slot_grid[None, :]).astype(jnp.bfloat16)
    to_slots = (select_first + select_second).T
    routes = group_prob[:, None] * pair_prob / jnp.sum(pair_prob, axis=1, keepdims=True)
    return feed(
        n_ep,
        n_tp,
        capacity,
        attended,
        tokens,
        ffn_gain,
        (output_weight, dense_gate_proj, dense_up_proj, dense_down_proj),
        dense_mix,
        (to_slots, select_first, select_second),
        routes,
        (expert_gate, expert_up, expert_down),
    )


def solution(mesh):
    return jax.shard_map(
        shards,
        mesh=mesh,
        in_specs=(
            P("ep", None),
            P(),
            P("ep", "tp"),
            P("ep", "tp"),
            P("ep", "tp"),
            P(None, "tp"),
            P("tp"),
            P("ep", "tp", None, None),
            P("ep", "tp", None, None),
            P("ep", "tp", None),
            P("ep"),
            P("tp", "ep"),
            P(),
            P("ep", "tp"),
            P("ep", "tp"),
            P("tp", "ep"),
            P(),
            P("ep", None),
            P("ep"),
            P("ep", None),
            P("ep", None, "tp"),
            P("ep", None, "tp"),
            P("ep", "tp", None),
        ),
        out_specs=P("ep", None),
        check_vma=False,
    )
```

```python
import functools
import math

import jax
import jax.numpy as jnp
from jax import lax
from jax.experimental import pallas as pl
from jax.experimental.pallas import tpu as pltpu
from jax.sharding import PartitionSpec as P

EPSILON = 1e-06


def rms_scale(values, norm_gain):
    widened = values.astype(jnp.float32)
    return (
        widened
        * lax.rsqrt(jnp.mean(widened * widened, axis=-1, keepdims=True) + EPSILON)
        * norm_gain
    )


MESH = pl.DeviceIdType.MESH
F32 = jnp.float32
BF16 = jnp.bfloat16


def fan_out(axis, count, me, source_of, landing, send_sem, recv_sem, slot=None):
    copies = []
    place = me if slot is None else slot(me)
    for step in range(1, count):
        target = lax.rem(me + step, count)
        copy = pltpu.make_async_remote_copy(
            src_ref=source_of(target),
            dst_ref=landing.at[place],
            send_sem=send_sem.at[step],
            recv_sem=recv_sem.at[me],
            device_id={axis: target},
            device_id_type=MESH,
        )
        copy.start()
        copies.append(copy)
    return copies


def collect(axis, count, me, landing, send_sem, recv_sem, slot=None):
    for step in range(1, count):
        source = lax.rem(me + count - step, count)
        place = source if slot is None else slot(source)
        pltpu.make_async_remote_copy(
            src_ref=landing.at[place],
            dst_ref=landing.at[place],
            send_sem=send_sem.at[step],
            recv_sem=recv_sem.at[source],
            device_id={axis: source},
            device_id_type=MESH,
        ).wait_recv()


def spread_rows(axis_ep, axis_tp, n_ep, n_tp, me_ep, me_tp, held, landing, send_sem, recv_sem):
    ratio = n_ep // n_tp
    for part in range(ratio):
        target_ep = me_tp * ratio + part
        for step in range(n_tp):
            target_tp = lax.rem(me_tp + step, n_tp)

            def send():
                pltpu.make_async_remote_copy(
                    src_ref=held.at[part],
                    dst_ref=landing.at[me_ep],
                    send_sem=send_sem.at[part * n_tp + step],
                    recv_sem=recv_sem.at[me_ep],
                    device_id={axis_ep: target_ep, axis_tp: target_tp},
                    device_id_type=MESH,
                ).start()

            if step == 0:
                pl.when(target_ep != me_ep)(send)

                @pl.when(target_ep == me_ep)
                def _():
                    landing[me_ep] = held[part]
            else:
                send()


def spread_wait(axis_ep, axis_tp, n_ep, n_tp, me_ep, me_tp, held, landing, send_sem, recv_sem):
    ratio = n_ep // n_tp
    own_tp = me_ep // ratio
    for step in range(n_ep):
        source = lax.rem(me_ep + n_ep - step, n_ep)

        def arrive():
            pltpu.make_async_remote_copy(
                src_ref=landing.at[source],
                dst_ref=landing.at[source],
                send_sem=send_sem.at[0],
                recv_sem=recv_sem.at[source],
                device_id={axis_ep: source, axis_tp: own_tp},
                device_id_type=MESH,
            ).wait_recv()

        if step == 0:
            pl.when(own_tp != me_tp)(arrive)
        else:
            arrive()


def spread_sent(axis_ep, axis_tp, n_ep, n_tp, me_ep, me_tp, held, landing, send_sem, recv_sem):
    ratio = n_ep // n_tp
    for part in range(ratio):
        target_ep = me_tp * ratio + part
        for step in range(n_tp):
            target_tp = lax.rem(me_tp + step, n_tp)

            def sent():
                pltpu.make_async_remote_copy(
                    src_ref=held.at[part],
                    dst_ref=landing.at[me_ep],
                    send_sem=send_sem.at[part * n_tp + step],
                    recv_sem=recv_sem.at[me_ep],
                    device_id={axis_ep: target_ep, axis_tp: target_tp},
                    device_id_type=MESH,
                ).wait_send()

            if step == 0:
                pl.when(target_ep != me_ep)(sent)
            else:
                sent()


def total_of(ref, count):
    total = ref[0].astype(F32)
    for index in range(1, count):
        total = total + ref[index].astype(F32)
    return total


def dot32(left, right):
    return jnp.dot(left, right, preferred_element_type=F32)


def chip_order(index, half):
    return lax.rem(index, 2) * half + index // 2


def pair_copy(axis, me, source, landing, send_sem, recv_sem, slot):
    return pltpu.make_async_remote_copy(
        src_ref=source,
        dst_ref=landing,
        send_sem=send_sem.at[slot],
        recv_sem=recv_sem.at[slot],
        device_id={axis: me + 1 - 2 * lax.rem(me, 2)},
        device_id_type=MESH,
    )


def chip_fan(axis, half, me, held, landing, send_sem, recv_sem):
    chip, core = me // 2, lax.rem(me, 2)
    copies = []
    for step in range(1, half):
        target = lax.rem(chip + step, half)
        copy = pltpu.make_async_remote_copy(
            src_ref=held.at[target],
            dst_ref=landing.at[chip],
            send_sem=send_sem.at[step],
            recv_sem=recv_sem.at[chip],
            device_id={axis: target * 2 + core},
            device_id_type=MESH,
        )
        copy.start()
        copies.append(copy)
    landing[chip] = held[chip]
    return copies


def chip_collect(axis, half, me, landing, send_sem, recv_sem):
    chip, core = me // 2, lax.rem(me, 2)
    for step in range(1, half):
        source = lax.rem(chip + half - step, half)
        pltpu.make_async_remote_copy(
            src_ref=landing.at[source],
            dst_ref=landing.at[source],
            send_sem=send_sem.at[step],
            recv_sem=recv_sem.at[source],
            device_id={axis: source * 2 + core},
            device_id_type=MESH,
        ).wait_recv()


def layer_kernel(
    n_ep,
    n_tp,
    forget_bias,
    tokens,
    attn_gain,
    forget_rows,
    gates,
    lengths,
    gain,
    dense_mix,
    to_slots,
    from_first,
    from_second,
    routes,
    query_weight,
    key_weight,
    value_weight,
    keys,
    values,
    output_weight,
    dense_gate,
    dense_up,
    expert_gate,
    expert_up,
    expert_down,
    dense_down,
    out,
    query_weight_held,
    key_weight_held,
    value_weight_held,
    keys_held,
    values_held,
    output_weight_held,
    dense_gate_held,
    dense_up_held,
    expert_gate_held,
    expert_up_held,
    expert_down_held,
    dense_down_held,
    load_sem,
    norm_send,
    norm_land,
    norm_ss,
    norm_rs,
    part_send,
    part_land,
    part_ss,
    part_rs,
    score_send,
    score_land,
    score_ss,
    score_rs,
    value_send,
    value_land,
    value_ss,
    value_rs,
    query_rows,
    key_rows,
    value_rows,
    forget_logs,
    scores,
    mixed,
    attended,
    full,
    att_land,
    att_ss,
    att_rs,
    head_send,
    head_land,
    head_ss,
    head_rs,
    mix_send,
    mix_land,
    mix_ss,
    mix_rs,
    ffn_send,
    ffn_land,
    ffn_ss,
    ffn_rs,
    slot_send,
    slot_land,
    slot_ss,
    slot_rs,
    pair_send,
    pair_land,
    pair_ss,
    pair_rs,
    dense_send,
    dense_land,
    dense_ss,
    dense_rs,
    expert_send,
    expert_land,
    expert_ss,
    expert_rs,
    back_send,
    back_land,
    back_ss,
    back_rs,
    hidden_send,
    hidden_land,
    hidden_ss,
    hidden_rs,
    down_send,
    down_land,
    down_ss,
    down_rs,
    tail_send,
    tail_land,
    tail_ss,
    tail_rs,
    route_send,
    route_land,
    route_ss,
    route_rs,
):
    me = lax.axis_index("ep")
    me_tp = lax.axis_index("tp")
    barrier = pltpu.get_barrier_semaphore()
    everyone = n_ep * n_tp
    place = me * n_tp + me_tp

    def greet(step, carry):
        other = lax.rem(place + step, everyone)
        pl.semaphore_signal(
            barrier,
            inc=1,
            device_id={"ep": other // n_tp, "tp": lax.rem(other, n_tp)},
            device_id_type=MESH,
        )
        return carry

    lax.fori_loop(1, everyone, greet, 0)
    sources = (query_weight, key_weight, value_weight, keys, values, output_weight, dense_gate, dense_up, expert_gate, expert_up, expert_down, dense_down)
    places = (query_weight_held, key_weight_held, value_weight_held, keys_held, values_held, output_weight_held, dense_gate_held, dense_up_held, expert_gate_held, expert_up_held, expert_down_held, dense_down_held)
    loads = [
        pltpu.make_async_copy(source, place, load_sem.at[index])
        for index, (source, place) in enumerate(zip(sources, places))
    ]
    for load in loads:
        load.start()
    rows, model = tokens.shape
    depth, hidden = query_weight.shape
    heads, span, size = keys.shape[1:]
    slots = slot_send.shape[1]
    group_rows = n_ep * rows // n_tp
    ratio = n_ep // n_tp
    half = n_ep // 2
    chip, core = me // 2, lax.rem(me, 2)
    grid = (n_ep, n_tp, me, me_tp)

    def order(index):
        return chip_order(index, half)

    normed = rms_scale(tokens[...], attn_gain[...])
    for index in range(n_ep):
        norm_send[index] = normed[:, index * depth : (index + 1) * depth].astype(BF16)
    pl.semaphore_wait(barrier, everyone - 1)

    sent = fan_out("ep", n_ep, me, lambda t: norm_send.at[t], norm_land, norm_ss, norm_rs, order)
    norm_land[order(me)] = norm_send[me]
    normed_wide = normed.astype(BF16).astype(F32)
    for head in range(heads):
        logit = forget_bias[0, head] + jnp.sum(
            normed_wide * forget_rows[head : head + 1, :].astype(F32), axis=-1, keepdims=True
        )
        forget_log = jnp.minimum(logit, 0.0) - jnp.log1p(jnp.exp(-jnp.abs(logit)))
        forget_logs[:, head, :] = jnp.broadcast_to(forget_log, (rows, size))
    collect("ep", n_ep, me, norm_land, norm_ss, norm_rs, order)
    joined = norm_land[...].reshape(n_ep * rows, depth)
    for index, weight in enumerate((query_weight_held, key_weight_held, value_weight_held)):
        loads[index].wait()
        part_send[:, :, :, index * hidden : (index + 1) * hidden] = dot32(
            joined, weight[...]
        ).reshape(2, half, rows, hidden)
    swap = pair_copy("ep", me, part_send.at[1 - core], part_land, part_ss, part_rs, 0)
    swap.start()
    swap.wait_recv()
    score_send[...] = part_send[core, :, :, : 2 * hidden] + part_land[:, :, : 2 * hidden]
    sent += chip_fan("ep", half, me, score_send, score_land, score_ss, score_rs)
    value_send[...] = (part_send[core, :, :, 2 * hidden :] + part_land[:, :, 2 * hidden :]).astype(
        BF16
    )
    sent += chip_fan("ep", half, me, value_send, value_land, value_ss, value_rs)
    sent.append(swap)
    chip_collect("ep", half, me, score_land, score_ss, score_rs)
    summed = total_of(score_land, half).astype(BF16).astype(F32)
    for head in range(heads):
        query_rows[:, head, :] = summed[:, head * size : (head + 1) * size]
        key_rows[:, head, :] = summed[:, hidden + head * size : hidden + (head + 1) * size]

    scale = 1.0 / math.sqrt(size)
    loads[3].wait()
    loads[4].wait()

    def score_step(seq, carry):
        for head in range(heads):
            query = query_rows[seq, head : head + 1, :].astype(BF16)
            scores[seq, head : head + 1, :] = lax.dot_general(
                query,
                keys_held[seq, head],
                (((1,), (1,)), ((), ())),
                preferred_element_type=F32,
            )
        return carry

    lax.fori_loop(0, rows, score_step, 0)
    positions = lax.broadcasted_iota(jnp.int32, (rows, heads, span), 2)
    lives = lengths[...]
    gate_all = gates[...]
    last_gate = jnp.sum(jnp.where(positions == lives - 1, gate_all, 0.0), axis=-1, keepdims=True)
    gate_now = last_gate + forget_logs[:, :, 0:1]
    score_all = scores[...] * scale + gate_now - gate_all
    score_all = jnp.where(positions < lives, score_all, -jnp.inf)
    own_score = jnp.sum(query_rows[...] * key_rows[...], axis=-1, keepdims=True) * scale
    row_top = jnp.maximum(jnp.max(score_all, axis=-1, keepdims=True), own_score)
    raised = jnp.exp(score_all - row_top)
    own_raised = jnp.exp(own_score - row_top)
    totals = jnp.sum(raised, axis=-1, keepdims=True) + own_raised
    scores[...] = raised / totals
    own_prob = (own_raised / totals).astype(BF16).astype(F32)

    def value_step(seq, carry):
        for head in range(heads):
            weight = scores[seq, head : head + 1, :].astype(BF16)
            mixed[seq, head : head + 1, :] = dot32(weight, values_held[seq, head])
        return carry

    lax.fori_loop(0, rows, value_step, 0)
    chip_collect("ep", half, me, value_land, value_ss, value_rs)
    value_sum = total_of(value_land, half).astype(BF16).astype(F32)
    for head in range(heads):
        value_rows[:, head, :] = value_sum[:, head * size : (head + 1) * size]
    mixed[...] = mixed[...] + own_prob * value_rows[...]
    for head in range(heads):
        attended[:, head * size : (head + 1) * size] = mixed[:, head, :].astype(BF16)

    sent += fan_out("ep", n_ep, me, lambda t: attended, att_land, att_ss, att_rs)
    att_land[me] = attended[...]
    collect("ep", n_ep, me, att_land, att_ss, att_rs)
    loads[5].wait()
    shares = dot32(att_land[...].reshape(n_ep * rows, hidden), output_weight_held[...])
    head_send[...] = shares.reshape(n_tp, group_rows, depth)
    sent += fan_out("tp", n_tp, me_tp, lambda t: head_send.at[t], head_land, head_ss, head_rs)
    head_land[me_tp] = head_send[me_tp]
    collect("tp", n_tp, me_tp, head_land, head_ss, head_rs)
    mix_send[...] = total_of(head_land, n_tp).reshape(ratio, rows, depth)
    spread_rows("ep", "tp", *grid, mix_send, mix_land, mix_ss, mix_rs)
    spread_wait("ep", "tp", *grid, mix_send, mix_land, mix_ss, mix_rs)
    for index in range(n_ep):
        full[:, index * depth : (index + 1) * depth] = mix_land[index]
    residual = (tokens[...].astype(F32) + full[...]).astype(BF16)
    ffn_wide = rms_scale(residual, gain[...])
    ffn_in = ffn_wide.astype(BF16)

    for index in range(n_ep):
        ffn_send[index] = ffn_wide[:, index * depth : (index + 1) * depth].astype(BF16)
    sent += fan_out("ep", n_ep, me, lambda t: ffn_send.at[t], ffn_land, ffn_ss, ffn_rs, order)
    outbound = dot32(to_slots[...], ffn_in)
    for index in range(n_ep):
        slot_send[index] = outbound[index * slots : (index + 1) * slots].astype(BF16)
    sent += fan_out("ep", n_ep, me, lambda t: slot_send.at[t], slot_land, slot_ss, slot_rs)
    ffn_land[order(me)] = ffn_send[me]
    slot_land[me] = slot_send[me]
    mix = jax.nn.sigmoid(
        jnp.sum(ffn_in.astype(F32) * dense_mix[...].astype(F32), axis=-1, keepdims=True)
    )

    collect("ep", n_ep, me, ffn_land, ffn_ss, ffn_rs, order)
    ffn_rows = ffn_land[...].reshape(n_ep * rows, depth)
    for index, weight in enumerate((dense_gate_held, dense_up_held)):
        loads[6 + index].wait()
        pair_send[:, :, :, index * hidden : (index + 1) * hidden] = dot32(
            ffn_rows, weight[...]
        ).reshape(2, half, rows, hidden)
    swap = pair_copy("ep", me, pair_send.at[1 - core], pair_land, pair_ss, pair_rs, 0)
    swap.start()
    swap.wait_recv()
    sent.append(swap)
    dense_send[...] = (pair_send[core] + pair_land[...]).astype(BF16)
    sent += chip_fan("ep", half, me, dense_send, dense_land, dense_ss, dense_rs)

    collect("ep", n_ep, me, slot_land, slot_ss, slot_rs)
    for load in loads[8:]:
        load.wait()
    slot_rows = jnp.concatenate(
        [slot_land[index].astype(F32) for index in range(n_ep)], axis=0
    ).astype(BF16)
    gate_part = dot32(slot_rows, expert_gate_held[0])
    up_part = dot32(slot_rows, expert_up_held[0])
    expert_hidden = (gate_part / (1.0 + jnp.exp(-gate_part)) * up_part).astype(BF16)
    chunk = model // n_tp
    for index in range(n_tp):
        expert_send[index] = dot32(
            expert_hidden, expert_down_held[0, :, index * chunk : (index + 1) * chunk]
        ).astype(BF16)
    sent += fan_out(
        "tp", n_tp, me_tp, lambda t: expert_send.at[t], expert_land, expert_ss, expert_rs
    )
    expert_land[me_tp] = expert_send[me_tp]

    chip_collect("ep", half, me, dense_land, dense_ss, dense_rs)
    dense_sum = total_of(dense_land, half)
    dense_first = dense_sum[:, :hidden]
    hidden_send[...] = (
        dense_first / (1.0 + jnp.exp(-dense_first)) * dense_sum[:, hidden:]
    ).astype(BF16)
    sent += fan_out("ep", n_ep, me, lambda t: hidden_send, hidden_land, hidden_ss, hidden_rs)
    hidden_land[me] = hidden_send[...]

    collect("tp", n_tp, me_tp, expert_land, expert_ss, expert_rs)
    expert_total = total_of(expert_land, n_tp)
    for index in range(n_ep):
        back_send[index] = expert_total[index * slots : (index + 1) * slots].astype(BF16)
    sent += fan_out("ep", n_ep, me, lambda t: back_send.at[t], back_land, back_ss, back_rs)
    back_land[me] = back_send[me]

    collect("ep", n_ep, me, hidden_land, hidden_ss, hidden_rs)
    down = dot32(hidden_land[...].reshape(n_ep * rows, hidden), dense_down_held[...])
    down_send[...] = down.astype(BF16).reshape(n_tp, group_rows, depth)
    sent += fan_out("tp", n_tp, me_tp, lambda t: down_send.at[t], down_land, down_ss, down_rs)
    down_land[me_tp] = down_send[me_tp]

    collect("ep", n_ep, me, back_land, back_ss, back_rs)
    back_rows = jnp.concatenate(
        [back_land[index].astype(F32) for index in range(n_ep)], axis=0
    ).astype(BF16)
    route_send[...] = routes[:, 0:1] * dot32(from_first[...], back_rows) + routes[:, 1:2] * dot32(
        from_second[...], back_rows
    )
    sent += fan_out("tp", n_tp, me_tp, lambda t: route_send, route_land, route_ss, route_rs)
    route_land[me_tp] = route_send[...]

    collect("tp", n_tp, me_tp, down_land, down_ss, down_rs)
    tail_send[...] = total_of(down_land, n_tp).astype(BF16).reshape(ratio, rows, depth)
    spread_rows("ep", "tp", *grid, tail_send, tail_land, tail_ss, tail_rs)
    collect("tp", n_tp, me_tp, route_land, route_ss, route_rs)
    spread_wait("ep", "tp", *grid, tail_send, tail_land, tail_ss, tail_rs)
    for index in range(n_ep):
        full[:, index * depth : (index + 1) * depth] = tail_land[index].astype(F32)
    for index in range(n_tp):
        span = slice(index * chunk, (index + 1) * chunk)
        out[:, span] = (
            residual[:, span].astype(F32) + route_land[index] + mix * full[:, span]
        ).astype(BF16)
    for copy in sent:
        copy.wait_send()
    spread_sent("ep", "tp", *grid, mix_send, mix_land, mix_ss, mix_rs)
    spread_sent("ep", "tp", *grid, tail_send, tail_land, tail_ss, tail_rs)


def layer(n_ep, n_tp, slots, forget_bias, small, large):
    rows, model = small[0].shape
    depth, hidden = large[0].shape
    heads, span, size = large[3].shape[1:]
    group_rows = n_ep * rows // n_tp
    ratio = n_ep // n_tp
    half = n_ep // 2
    chunk = model // n_tp
    vmem = pl.BlockSpec(memory_space=pltpu.VMEM)
    smem = pl.BlockSpec(memory_space=pltpu.SMEM)
    hbm = pl.BlockSpec(memory_space=pltpu.HBM)
    return pl.pallas_call(
        functools.partial(layer_kernel, n_ep, n_tp),
        out_shape=jax.ShapeDtypeStruct((rows, model), BF16),
        in_specs=[smem] + [vmem] * len(small) + [hbm] * len(large),
        out_specs=vmem,
        scratch_shapes=[
            pltpu.VMEM(large[0].shape, BF16),
            pltpu.VMEM(large[1].shape, BF16),
            pltpu.VMEM(large[2].shape, BF16),
            pltpu.VMEM(large[3].shape, BF16),
            pltpu.VMEM(large[4].shape, BF16),
            pltpu.VMEM(large[5].shape, BF16),
            pltpu.VMEM(large[6].shape, BF16),
            pltpu.VMEM(large[7].shape, BF16),
            pltpu.VMEM(large[8].shape, BF16),
            pltpu.VMEM(large[9].shape, BF16),
            pltpu.VMEM(large[10].shape, BF16),
            pltpu.VMEM(large[11].shape, BF16),
            pltpu.SemaphoreType.DMA((12,)),
            pltpu.VMEM((n_ep, rows, depth), BF16),
            pltpu.VMEM((n_ep, rows, depth), BF16),
            pltpu.SemaphoreType.DMA((n_ep,)),
            pltpu.SemaphoreType.DMA((n_ep,)),
            pltpu.VMEM((2, half, rows, 3 * hidden), F32),
            pltpu.VMEM((half, rows, 3 * hidden), F32),
            pltpu.SemaphoreType.DMA((1,)),
            pltpu.SemaphoreType.DMA((1,)),
            pltpu.VMEM((half, rows, 2 * hidden), F32),
            pltpu.VMEM((half, rows, 2 * hidden), F32),
            pltpu.SemaphoreType.DMA((half,)),
            pltpu.SemaphoreType.DMA((half,)),
            pltpu.VMEM((half, rows, hidden), BF16),
            pltpu.VMEM((half, rows, hidden), BF16),
            pltpu.SemaphoreType.DMA((half,)),
            pltpu.SemaphoreType.DMA((half,)),
            pltpu.VMEM((rows, heads, size), F32),
            pltpu.VMEM((rows, heads, size), F32),
            pltpu.VMEM((rows, heads, size), F32),
            pltpu.VMEM((rows, heads, size), F32),
            pltpu.VMEM((rows, heads, span), F32),
            pltpu.VMEM((rows, heads, size), F32),
            pltpu.VMEM((rows, hidden), BF16),
            pltpu.VMEM((rows, model), F32),
            pltpu.VMEM((n_ep, rows, hidden), BF16),
            pltpu.SemaphoreType.DMA((n_ep,)),
            pltpu.SemaphoreType.DMA((n_ep,)),
            pltpu.VMEM((n_tp, group_rows, depth), F32),
            pltpu.VMEM((n_tp, group_rows, depth), F32),
            pltpu.SemaphoreType.DMA((n_tp,)),
            pltpu.SemaphoreType.DMA((n_tp,)),
            pltpu.VMEM((ratio, rows, depth), F32),
            pltpu.VMEM((n_ep, rows, depth), F32),
            pltpu.SemaphoreType.DMA((n_ep,)),
            pltpu.SemaphoreType.DMA((n_ep,)),
            pltpu.VMEM((n_ep, rows, depth), BF16),
            pltpu.VMEM((n_ep, rows, depth), BF16),
            pltpu.SemaphoreType.DMA((n_ep,)),
            pltpu.SemaphoreType.DMA((n_ep,)),
            pltpu.VMEM((n_ep, slots, model), BF16),
            pltpu.VMEM((n_ep, slots, model), BF16),
            pltpu.SemaphoreType.DMA((n_ep,)),
            pltpu.SemaphoreType.DMA((n_ep,)),
            pltpu.VMEM((2, half, rows, 2 * hidden), F32),
            pltpu.VMEM((half, rows, 2 * hidden), F32),
            pltpu.SemaphoreType.DMA((1,)),
            pltpu.SemaphoreType.DMA((1,)),
            pltpu.VMEM((half, rows, 2 * hidden), BF16),
            pltpu.VMEM((half, rows, 2 * hidden), BF16),
            pltpu.SemaphoreType.DMA((half,)),
            pltpu.SemaphoreType.DMA((half,)),
            pltpu.VMEM((n_tp, n_ep * slots, chunk), BF16),
            pltpu.VMEM((n_tp, n_ep * slots, chunk), BF16),
            pltpu.SemaphoreType.DMA((n_tp,)),
            pltpu.SemaphoreType.DMA((n_tp,)),
            pltpu.VMEM((n_ep, slots, chunk), BF16),
            pltpu.VMEM((n_ep, slots, chunk), BF16),
            pltpu.SemaphoreType.DMA((n_ep,)),
            pltpu.SemaphoreType.DMA((n_ep,)),
            pltpu.VMEM((rows, hidden), BF16),
            pltpu.VMEM((n_ep, rows, hidden), BF16),
            pltpu.SemaphoreType.DMA((n_ep,)),
            pltpu.SemaphoreType.DMA((n_ep,)),
            pltpu.VMEM((n_tp, group_rows, depth), BF16),
            pltpu.VMEM((n_tp, group_rows, depth), BF16),
            pltpu.SemaphoreType.DMA((n_tp,)),
            pltpu.SemaphoreType.DMA((n_tp,)),
            pltpu.VMEM((ratio, rows, depth), BF16),
            pltpu.VMEM((n_ep, rows, depth), BF16),
            pltpu.SemaphoreType.DMA((n_ep,)),
            pltpu.SemaphoreType.DMA((n_ep,)),
            pltpu.VMEM((rows, chunk), F32),
            pltpu.VMEM((n_tp, rows, chunk), F32),
            pltpu.SemaphoreType.DMA((n_tp,)),
            pltpu.SemaphoreType.DMA((n_tp,)),
        ],
        compiler_params=pltpu.CompilerParams(
            collective_id=0, has_side_effects=True, vmem_limit_bytes=60 * 1024 * 1024
        ),
    )(forget_bias, *small, *large)


def shards(
    tokens,
    attn_gain,
    query_weight,
    key_weight,
    value_weight,
    forget_weight,
    forget_bias,
    cache_keys,
    cache_values,
    cache_gates,
    lengths,
    output_weight,
    ffn_gain,
    dense_gate_proj,
    dense_up_proj,
    dense_down_proj,
    dense_mix,
    expert_ids,
    group_prob,
    pair_prob,
    expert_gate,
    expert_up,
    expert_down,
):
    seq_count = tokens.shape[0]
    n_ep = lax.axis_size("ep")
    n_tp = lax.axis_size("tp")
    expert_count = n_ep * expert_gate.shape[0]
    capacity = max(4 * seq_count // expert_count, 8)
    slot_total = expert_count * capacity
    picks = expert_ids.reshape(-1)
    same = (picks[:, None] == picks[None, :]).astype(jnp.int32)
    before = jnp.tril(jnp.ones((2 * seq_count, 2 * seq_count), jnp.int32), -1)
    slot_rank = jnp.sum(same * before, axis=1)
    destination = (picks * capacity + slot_rank).reshape(seq_count, 2)
    slot_grid = jnp.arange(slot_total, dtype=jnp.int32)
    select_first = (destination[:, 0:1] == slot_grid[None, :]).astype(jnp.bfloat16)
    select_second = (destination[:, 1:2] == slot_grid[None, :]).astype(jnp.bfloat16)
    to_slots = (select_first + select_second).T
    routes = group_prob[:, None] * pair_prob / jnp.sum(pair_prob, axis=1, keepdims=True)
    model = (1, tokens.shape[1])
    return layer(
        n_ep,
        n_tp,
        capacity,
        forget_bias.reshape(1, -1),
        (
            tokens,
            attn_gain.reshape(model),
            forget_weight.T,
            cache_gates,
            lengths.reshape(-1, 1, 1),
            ffn_gain.reshape(model),
            dense_mix.reshape(model),
            to_slots,
            select_first,
            select_second,
            routes,
        ),
        (
            query_weight,
            key_weight,
            value_weight,
            cache_keys,
            cache_values,
            output_weight,
            dense_gate_proj,
            dense_up_proj,
            expert_gate,
            expert_up,
            expert_down,
            dense_down_proj,
        ),
    )


def solution(mesh):
    return jax.shard_map(
        shards,
        mesh=mesh,
        in_specs=(
            P("ep", None),
            P(),
            P("ep", "tp"),
            P("ep", "tp"),
            P("ep", "tp"),
            P(None, "tp"),
            P("tp"),
            P("ep", "tp", None, None),
            P("ep", "tp", None, None),
            P("ep", "tp", None),
            P("ep"),
            P("tp", "ep"),
            P(),
            P("ep", "tp"),
            P("ep", "tp"),
            P("tp", "ep"),
            P(),
            P("ep", None),
            P("ep"),
            P("ep", None),
            P("ep", None, "tp"),
            P("ep", None, "tp"),
            P("ep", "tp", None),
        ),
        out_specs=P("ep", None),
        check_vma=False,
    )
```

```python
import functools
import math

import jax
import jax.numpy as jnp
from jax import lax
from jax.experimental import pallas as pl
from jax.experimental.pallas import tpu as pltpu
from jax.sharding import PartitionSpec as P

EPSILON = 1e-06


def rms_scale(values, norm_gain):
    widened = values.astype(jnp.float32)
    return (
        widened
        * lax.rsqrt(jnp.mean(widened * widened, axis=-1, keepdims=True) + EPSILON)
        * norm_gain
    )


MESH = pl.DeviceIdType.MESH
F32 = jnp.float32
BF16 = jnp.bfloat16


def fan_out(axis, count, me, source_of, landing, send_sem, recv_sem, slot=None):
    copies = []
    place = me if slot is None else slot(me)
    for step in range(1, count):
        target = lax.rem(me + step, count)
        copy = pltpu.make_async_remote_copy(
            src_ref=source_of(target),
            dst_ref=landing.at[place],
            send_sem=send_sem.at[step],
            recv_sem=recv_sem.at[me],
            device_id={axis: target},
            device_id_type=MESH,
        )
        copy.start()
        copies.append(copy)
    return copies


def collect(axis, count, me, landing, send_sem, recv_sem, slot=None):
    for step in range(1, count):
        source = lax.rem(me + count - step, count)
        place = source if slot is None else slot(source)
        pltpu.make_async_remote_copy(
            src_ref=landing.at[place],
            dst_ref=landing.at[place],
            send_sem=send_sem.at[step],
            recv_sem=recv_sem.at[source],
            device_id={axis: source},
            device_id_type=MESH,
        ).wait_recv()


def spread_rows(axis_ep, axis_tp, n_ep, n_tp, me_ep, me_tp, held, landing, send_sem, recv_sem):
    ratio = n_ep // n_tp
    for part in range(ratio):
        target_ep = me_tp * ratio + part
        for step in range(n_tp):
            target_tp = lax.rem(me_tp + step, n_tp)

            def send():
                pltpu.make_async_remote_copy(
                    src_ref=held.at[part],
                    dst_ref=landing.at[me_ep],
                    send_sem=send_sem.at[part * n_tp + step],
                    recv_sem=recv_sem.at[me_ep],
                    device_id={axis_ep: target_ep, axis_tp: target_tp},
                    device_id_type=MESH,
                ).start()

            if step == 0:
                pl.when(target_ep != me_ep)(send)

                @pl.when(target_ep == me_ep)
                def _():
                    landing[me_ep] = held[part]
            else:
                send()


def spread_wait(axis_ep, axis_tp, n_ep, n_tp, me_ep, me_tp, held, landing, send_sem, recv_sem):
    ratio = n_ep // n_tp
    own_tp = me_ep // ratio
    for step in range(n_ep):
        source = lax.rem(me_ep + n_ep - step, n_ep)

        def arrive():
            pltpu.make_async_remote_copy(
                src_ref=landing.at[source],
                dst_ref=landing.at[source],
                send_sem=send_sem.at[0],
                recv_sem=recv_sem.at[source],
                device_id={axis_ep: source, axis_tp: own_tp},
                device_id_type=MESH,
            ).wait_recv()

        if step == 0:
            pl.when(own_tp != me_tp)(arrive)
        else:
            arrive()


def spread_sent(axis_ep, axis_tp, n_ep, n_tp, me_ep, me_tp, held, landing, send_sem, recv_sem):
    ratio = n_ep // n_tp
    for part in range(ratio):
        target_ep = me_tp * ratio + part
        for step in range(n_tp):
            target_tp = lax.rem(me_tp + step, n_tp)

            def sent():
                pltpu.make_async_remote_copy(
                    src_ref=held.at[part],
                    dst_ref=landing.at[me_ep],
                    send_sem=send_sem.at[part * n_tp + step],
                    recv_sem=recv_sem.at[me_ep],
                    device_id={axis_ep: target_ep, axis_tp: target_tp},
                    device_id_type=MESH,
                ).wait_send()

            if step == 0:
                pl.when(target_ep != me_ep)(sent)
            else:
                sent()


def total_of(ref, count):
    total = ref[0].astype(F32)
    for index in range(1, count):
        total = total + ref[index].astype(F32)
    return total


def dot32(left, right):
    return jnp.dot(left, right, preferred_element_type=F32)


def chip_order(index, half):
    return lax.rem(index, 2) * half + index // 2


def pair_copy(axis, me, source, landing, send_sem, recv_sem, slot):
    return pltpu.make_async_remote_copy(
        src_ref=source,
        dst_ref=landing,
        send_sem=send_sem.at[slot],
        recv_sem=recv_sem.at[slot],
        device_id={axis: me + 1 - 2 * lax.rem(me, 2)},
        device_id_type=MESH,
    )


def chip_fan(axis, half, me, held, landing, send_sem, recv_sem):
    chip, core = me // 2, lax.rem(me, 2)
    copies = []
    for step in range(1, half):
        target = lax.rem(chip + step, half)
        copy = pltpu.make_async_remote_copy(
            src_ref=held.at[target],
            dst_ref=landing.at[chip],
            send_sem=send_sem.at[step],
            recv_sem=recv_sem.at[chip],
            device_id={axis: target * 2 + core},
            device_id_type=MESH,
        )
        copy.start()
        copies.append(copy)
    landing[chip] = held[chip]
    return copies


def chip_collect(axis, half, me, landing, send_sem, recv_sem):
    chip, core = me // 2, lax.rem(me, 2)
    for step in range(1, half):
        source = lax.rem(chip + half - step, half)
        pltpu.make_async_remote_copy(
            src_ref=landing.at[source],
            dst_ref=landing.at[source],
            send_sem=send_sem.at[step],
            recv_sem=recv_sem.at[source],
            device_id={axis: source * 2 + core},
            device_id_type=MESH,
        ).wait_recv()


def layer_kernel(
    n_ep,
    n_tp,
    forget_bias,
    lengths,
    tokens,
    attn_gain,
    forget_rows,
    gates,
    gain,
    gain_parts,
    dense_mix,
    to_slots,
    from_first,
    from_second,
    routes,
    query_weight,
    key_weight,
    value_weight,
    keys,
    values,
    output_weight,
    dense_gate,
    dense_up,
    expert_gate,
    expert_up,
    expert_down,
    dense_down,
    out,
    query_weight_held,
    key_weight_held,
    value_weight_held,
    keys_held,
    values_held,
    output_weight_held,
    dense_gate_held,
    dense_up_held,
    expert_gate_held,
    expert_up_held,
    expert_down_held,
    dense_down_held,
    load_sem,
    norm_send,
    norm_land,
    norm_ss,
    norm_rs,
    part_send,
    part_land,
    part_ss,
    part_rs,
    score_send,
    score_land,
    score_ss,
    score_rs,
    value_send,
    value_land,
    value_ss,
    value_rs,
    query_rows,
    key_rows,
    value_rows,
    forget_logs,
    scores,
    mixed,
    attended,
    full,
    att_land,
    att_ss,
    att_rs,
    head_send,
    head_land,
    head_ss,
    head_rs,
    mix_send,
    mix_land,
    mix_ss,
    mix_rs,
    token_send,
    token_land,
    token_ss,
    token_rs,
    share_land,
    share_ss,
    share_rs,
    slot_send,
    slot_land,
    slot_ss,
    slot_rs,
    pair_send,
    pair_land,
    pair_ss,
    pair_rs,
    dense_send,
    dense_land,
    dense_ss,
    dense_rs,
    expert_send,
    expert_land,
    expert_ss,
    expert_rs,
    back_send,
    back_land,
    back_ss,
    back_rs,
    hidden_send,
    hidden_land,
    hidden_ss,
    hidden_rs,
    down_send,
    down_land,
    down_ss,
    down_rs,
    tail_send,
    tail_land,
    tail_ss,
    tail_rs,
    route_send,
    route_land,
    route_ss,
    route_rs,
):
    me = lax.axis_index("ep")
    me_tp = lax.axis_index("tp")
    barrier = pltpu.get_barrier_semaphore()
    everyone = n_ep * n_tp
    place = me * n_tp + me_tp

    def greet(step, carry):
        other = lax.rem(place + step, everyone)
        pl.semaphore_signal(
            barrier,
            inc=1,
            device_id={"ep": other // n_tp, "tp": lax.rem(other, n_tp)},
            device_id_type=MESH,
        )
        return carry

    lax.fori_loop(1, everyone, greet, 0)
    sources = (query_weight, key_weight, value_weight, keys, values, output_weight, dense_gate, dense_up, expert_gate, expert_up, expert_down, dense_down)
    places = (query_weight_held, key_weight_held, value_weight_held, keys_held, values_held, output_weight_held, dense_gate_held, dense_up_held, expert_gate_held, expert_up_held, expert_down_held, dense_down_held)
    loads = [
        pltpu.make_async_copy(source, place, load_sem.at[index])
        for index, (source, place) in enumerate(zip(sources, places))
    ]
    for load in loads:
        load.start()
    rows, model = tokens.shape
    depth, hidden = query_weight.shape
    heads, span, size = keys.shape[1:]
    slots = slot_send.shape[1]
    group_rows = n_ep * rows // n_tp
    ratio = n_ep // n_tp
    half = n_ep // 2
    chip, core = me // 2, lax.rem(me, 2)
    grid = (n_ep, n_tp, me, me_tp)

    def order(index):
        return chip_order(index, half)

    normed = rms_scale(tokens[...], attn_gain[...])
    for index in range(n_ep):
        norm_send[index] = normed[:, index * depth : (index + 1) * depth].astype(BF16)
        token_send[index] = tokens[:, index * depth : (index + 1) * depth]
    pl.semaphore_wait(barrier, everyone - 1)

    sent = fan_out("ep", n_ep, me, lambda t: norm_send.at[t], norm_land, norm_ss, norm_rs, order)
    norm_land[order(me)] = norm_send[me]
    normed_wide = normed.astype(BF16).astype(F32)
    for head in range(heads):
        logit = forget_bias[0, head] + jnp.sum(
            normed_wide * forget_rows[head : head + 1, :].astype(F32), axis=-1, keepdims=True
        )
        forget_log = jnp.minimum(logit, 0.0) - jnp.log1p(jnp.exp(-jnp.abs(logit)))
        forget_logs[:, head, :] = jnp.broadcast_to(forget_log, (rows, size))
    collect("ep", n_ep, me, norm_land, norm_ss, norm_rs, order)
    joined = norm_land[...].reshape(n_ep * rows, depth)
    for index, weight in enumerate((query_weight_held, key_weight_held, value_weight_held)):
        loads[index].wait()
        part_send[:, :, :, index * hidden : (index + 1) * hidden] = dot32(
            joined, weight[...]
        ).reshape(2, half, rows, hidden)
    swap = pair_copy("ep", me, part_send.at[1 - core], part_land, part_ss, part_rs, 0)
    swap.start()
    swap.wait_recv()
    score_send[...] = part_send[core, :, :, : 2 * hidden] + part_land[:, :, : 2 * hidden]
    sent += chip_fan("ep", half, me, score_send, score_land, score_ss, score_rs)
    value_send[...] = (part_send[core, :, :, 2 * hidden :] + part_land[:, :, 2 * hidden :]).astype(
        BF16
    )
    sent += chip_fan("ep", half, me, value_send, value_land, value_ss, value_rs)
    sent.append(swap)
    sent += fan_out("ep", n_ep, me, lambda t: token_send.at[t], token_land, token_ss, token_rs)
    token_land[me] = token_send[me]
    chip_collect("ep", half, me, score_land, score_ss, score_rs)
    summed = total_of(score_land, half).astype(BF16).astype(F32)
    for head in range(heads):
        query_rows[:, head, :] = summed[:, head * size : (head + 1) * size]
        key_rows[:, head, :] = summed[:, hidden + head * size : hidden + (head + 1) * size]

    scale = 1.0 / math.sqrt(size)
    loads[3].wait()
    loads[4].wait()

    def score_step(seq, carry):
        for head in range(heads):
            query = query_rows[seq, head : head + 1, :].astype(BF16)
            scores[seq, head : head + 1, :] = lax.dot_general(
                query,
                keys_held[seq, head],
                (((1,), (1,)), ((), ())),
                preferred_element_type=F32,
            )
        return carry

    lax.fori_loop(0, rows, score_step, 0, unroll=4)
    positions = lax.broadcasted_iota(jnp.int32, (rows, heads, span), 2)
    sequences = lax.broadcasted_iota(jnp.int32, (rows, heads, size), 0)
    live_wide = jnp.zeros((rows, heads, size), jnp.int32)
    for seq in range(rows):
        live_wide = jnp.where(sequences == seq, lengths[0, seq], live_wide)
    lives = live_wide[:, :, 0:1]
    gate_all = gates[...]
    last_gate = jnp.sum(jnp.where(positions == lives - 1, gate_all, 0.0), axis=-1, keepdims=True)
    gate_now = last_gate + forget_logs[:, :, 0:1]
    score_all = scores[...] * scale + gate_now - gate_all
    score_all = jnp.where(positions < lives, score_all, -jnp.inf)
    own_score = jnp.sum(query_rows[...] * key_rows[...], axis=-1, keepdims=True) * scale
    row_top = jnp.maximum(jnp.max(score_all, axis=-1, keepdims=True), own_score)
    raised = jnp.exp(score_all - row_top)
    own_raised = jnp.exp(own_score - row_top)
    totals = jnp.sum(raised, axis=-1, keepdims=True) + own_raised
    scores[...] = raised / totals
    own_prob = (own_raised / totals).astype(BF16).astype(F32)

    def value_step(seq, carry):
        for head in range(heads):
            weight = scores[seq, head : head + 1, :].astype(BF16)
            mixed[seq, head : head + 1, :] = dot32(weight, values_held[seq, head])
        return carry

    lax.fori_loop(0, rows, value_step, 0, unroll=4)
    chip_collect("ep", half, me, value_land, value_ss, value_rs)
    value_sum = total_of(value_land, half).astype(BF16).astype(F32)
    for head in range(heads):
        value_rows[:, head, :] = value_sum[:, head * size : (head + 1) * size]
    mixed[...] = mixed[...] + own_prob * value_rows[...]
    for head in range(heads):
        attended[:, head * size : (head + 1) * size] = mixed[:, head, :].astype(BF16)

    sent += fan_out("ep", n_ep, me, lambda t: attended, att_land, att_ss, att_rs)
    att_land[me] = attended[...]
    collect("ep", n_ep, me, att_land, att_ss, att_rs)
    loads[5].wait()
    shares = dot32(att_land[...].reshape(n_ep * rows, hidden), output_weight_held[...])
    head_send[...] = shares.reshape(n_tp, group_rows, depth)
    sent += fan_out("tp", n_tp, me_tp, lambda t: head_send.at[t], head_land, head_ss, head_rs)
    head_land[me_tp] = head_send[me_tp]
    collect("tp", n_tp, me_tp, head_land, head_ss, head_rs)
    mix_send[...] = total_of(head_land, n_tp).reshape(ratio, rows, depth)
    spread_rows("ep", "tp", *grid, mix_send, mix_land, mix_ss, mix_rs)
    sent += fan_out("tp", n_tp, me_tp, lambda t: mix_send, share_land, share_ss, share_rs)
    share_land[me_tp] = mix_send[...]
    collect("ep", n_ep, me, token_land, token_ss, token_rs)
    collect("tp", n_tp, me_tp, share_land, share_ss, share_rs)

    shared = share_land[...].reshape(n_ep, rows, depth)
    residual_part = (token_land[...].astype(F32) + shared).astype(BF16)
    dense_rows = (residual_part.astype(F32) * gain_parts[me]).astype(BF16)
    dense_rows = dense_rows.reshape(n_ep * rows, depth)
    for index, weight in enumerate((dense_gate_held, dense_up_held)):
        loads[6 + index].wait()
        product = dot32(dense_rows, weight[...])
        for place in range(n_ep):
            pair_send[place % 2, place // 2, :, index * hidden : (index + 1) * hidden] = product[
                place * rows : (place + 1) * rows
            ]
    swap = pair_copy("ep", me, pair_send.at[1 - core], pair_land, pair_ss, pair_rs, 0)
    swap.start()
    swap.wait_recv()
    sent.append(swap)
    dense_send[...] = (pair_send[core] + pair_land[...]).astype(BF16)
    sent += chip_fan("ep", half, me, dense_send, dense_land, dense_ss, dense_rs)

    spread_wait("ep", "tp", *grid, mix_send, mix_land, mix_ss, mix_rs)
    for index in range(n_ep):
        full[:, index * depth : (index + 1) * depth] = mix_land[index]
    residual = (tokens[...].astype(F32) + full[...]).astype(BF16)
    residual_wide = residual.astype(F32)
    row_scale = lax.rsqrt(
        jnp.mean(residual_wide * residual_wide, axis=-1, keepdims=True) + EPSILON
    )
    ffn_in = (residual_wide * row_scale * gain[...]).astype(BF16)

    outbound = dot32(to_slots[...], ffn_in)
    for index in range(n_ep):
        slot_send[index] = outbound[index * slots : (index + 1) * slots].astype(BF16)
    sent += fan_out("ep", n_ep, me, lambda t: slot_send.at[t], slot_land, slot_ss, slot_rs)
    slot_land[me] = slot_send[me]
    mix = jax.nn.sigmoid(
        jnp.sum(ffn_in.astype(F32) * dense_mix[...].astype(F32), axis=-1, keepdims=True)
    )

    chip_collect("ep", half, me, dense_land, dense_ss, dense_rs)
    dense_sum = total_of(dense_land, half) * row_scale
    dense_first = dense_sum[:, :hidden]
    hidden_send[...] = (
        dense_first / (1.0 + jnp.exp(-dense_first)) * dense_sum[:, hidden:]
    ).astype(BF16)
    sent += fan_out("ep", n_ep, me, lambda t: hidden_send, hidden_land, hidden_ss, hidden_rs)
    hidden_land[me] = hidden_send[...]

    collect("ep", n_ep, me, slot_land, slot_ss, slot_rs)
    for load in loads[8:]:
        load.wait()
    slot_rows = jnp.concatenate(
        [slot_land[index].astype(F32) for index in range(n_ep)], axis=0
    ).astype(BF16)
    gate_part = dot32(slot_rows, expert_gate_held[0])
    up_part = dot32(slot_rows, expert_up_held[0])
    expert_hidden = (gate_part / (1.0 + jnp.exp(-gate_part)) * up_part).astype(BF16)
    chunk = model // n_tp
    for index in range(n_tp):
        expert_send[index] = dot32(
            expert_hidden, expert_down_held[0, :, index * chunk : (index + 1) * chunk]
        ).astype(BF16)
    sent += fan_out(
        "tp", n_tp, me_tp, lambda t: expert_send.at[t], expert_land, expert_ss, expert_rs
    )
    expert_land[me_tp] = expert_send[me_tp]

    collect("tp", n_tp, me_tp, expert_land, expert_ss, expert_rs)
    expert_total = total_of(expert_land, n_tp)
    for index in range(n_ep):
        back_send[index] = expert_total[index * slots : (index + 1) * slots].astype(BF16)
    sent += fan_out("ep", n_ep, me, lambda t: back_send.at[t], back_land, back_ss, back_rs)
    back_land[me] = back_send[me]

    collect("ep", n_ep, me, hidden_land, hidden_ss, hidden_rs)
    down = dot32(hidden_land[...].reshape(n_ep * rows, hidden), dense_down_held[...])
    down_send[...] = down.astype(BF16).reshape(n_tp, group_rows, depth)
    sent += fan_out("tp", n_tp, me_tp, lambda t: down_send.at[t], down_land, down_ss, down_rs)
    down_land[me_tp] = down_send[me_tp]

    collect("ep", n_ep, me, back_land, back_ss, back_rs)
    back_rows = jnp.concatenate(
        [back_land[index].astype(F32) for index in range(n_ep)], axis=0
    ).astype(BF16)
    route_send[...] = routes[:, 0:1] * dot32(from_first[...], back_rows) + routes[:, 1:2] * dot32(
        from_second[...], back_rows
    )
    sent += fan_out("tp", n_tp, me_tp, lambda t: route_send, route_land, route_ss, route_rs)
    route_land[me_tp] = route_send[...]

    collect("tp", n_tp, me_tp, down_land, down_ss, down_rs)
    tail_send[...] = total_of(down_land, n_tp).astype(BF16).reshape(ratio, rows, depth)
    spread_rows("ep", "tp", *grid, tail_send, tail_land, tail_ss, tail_rs)
    collect("tp", n_tp, me_tp, route_land, route_ss, route_rs)
    spread_wait("ep", "tp", *grid, tail_send, tail_land, tail_ss, tail_rs)
    for index in range(n_ep):
        full[:, index * depth : (index + 1) * depth] = tail_land[index].astype(F32)
    for index in range(n_tp):
        span = slice(index * chunk, (index + 1) * chunk)
        out[:, span] = (
            residual[:, span].astype(F32) + route_land[index] + mix * full[:, span]
        ).astype(BF16)
    for copy in sent:
        copy.wait_send()
    spread_sent("ep", "tp", *grid, mix_send, mix_land, mix_ss, mix_rs)
    spread_sent("ep", "tp", *grid, tail_send, tail_land, tail_ss, tail_rs)


def layer(n_ep, n_tp, slots, scalars, small, large):
    rows, model = small[0].shape
    depth, hidden = large[0].shape
    heads, span, size = large[3].shape[1:]
    group_rows = n_ep * rows // n_tp
    ratio = n_ep // n_tp
    half = n_ep // 2
    chunk = model // n_tp
    vmem = pl.BlockSpec(memory_space=pltpu.VMEM)
    smem = pl.BlockSpec(memory_space=pltpu.SMEM)
    hbm = pl.BlockSpec(memory_space=pltpu.HBM)
    return pl.pallas_call(
        functools.partial(layer_kernel, n_ep, n_tp),
        out_shape=jax.ShapeDtypeStruct((rows, model), BF16),
        in_specs=[smem] * 2 + [vmem] * len(small) + [hbm] * len(large),
        out_specs=vmem,
        scratch_shapes=[
            pltpu.VMEM(large[0].shape, BF16),
            pltpu.VMEM(large[1].shape, BF16),
            pltpu.VMEM(large[2].shape, BF16),
            pltpu.VMEM(large[3].shape, BF16),
            pltpu.VMEM(large[4].shape, BF16),
            pltpu.VMEM(large[5].shape, BF16),
            pltpu.VMEM(large[6].shape, BF16),
            pltpu.VMEM(large[7].shape, BF16),
            pltpu.VMEM(large[8].shape, BF16),
            pltpu.VMEM(large[9].shape, BF16),
            pltpu.VMEM(large[10].shape, BF16),
            pltpu.VMEM(large[11].shape, BF16),
            pltpu.SemaphoreType.DMA((12,)),
            pltpu.VMEM((n_ep, rows, depth), BF16),
            pltpu.VMEM((n_ep, rows, depth), BF16),
            pltpu.SemaphoreType.DMA((n_ep,)),
            pltpu.SemaphoreType.DMA((n_ep,)),
            pltpu.VMEM((2, half, rows, 3 * hidden), F32),
            pltpu.VMEM((half, rows, 3 * hidden), F32),
            pltpu.SemaphoreType.DMA((1,)),
            pltpu.SemaphoreType.DMA((1,)),
            pltpu.VMEM((half, rows, 2 * hidden), F32),
            pltpu.VMEM((half, rows, 2 * hidden), F32),
            pltpu.SemaphoreType.DMA((half,)),
            pltpu.SemaphoreType.DMA((half,)),
            pltpu.VMEM((half, rows, hidden), BF16),
            pltpu.VMEM((half, rows, hidden), BF16),
            pltpu.SemaphoreType.DMA((half,)),
            pltpu.SemaphoreType.DMA((half,)),
            pltpu.VMEM((rows, heads, size), F32),
            pltpu.VMEM((rows, heads, size), F32),
            pltpu.VMEM((rows, heads, size), F32),
            pltpu.VMEM((rows, heads, size), F32),
            pltpu.VMEM((rows, heads, span), F32),
            pltpu.VMEM((rows, heads, size), F32),
            pltpu.VMEM((rows, hidden), BF16),
            pltpu.VMEM((rows, model), F32),
            pltpu.VMEM((n_ep, rows, hidden), BF16),
            pltpu.SemaphoreType.DMA((n_ep,)),
            pltpu.SemaphoreType.DMA((n_ep,)),
            pltpu.VMEM((n_tp, group_rows, depth), F32),
            pltpu.VMEM((n_tp, group_rows, depth), F32),
            pltpu.SemaphoreType.DMA((n_tp,)),
            pltpu.SemaphoreType.DMA((n_tp,)),
            pltpu.VMEM((ratio, rows, depth), F32),
            pltpu.VMEM((n_ep, rows, depth), F32),
            pltpu.SemaphoreType.DMA((n_ep,)),
            pltpu.SemaphoreType.DMA((n_ep,)),
            pltpu.VMEM((n_ep, rows, depth), BF16),
            pltpu.VMEM((n_ep, rows, depth), BF16),
            pltpu.SemaphoreType.DMA((n_ep,)),
            pltpu.SemaphoreType.DMA((n_ep,)),
            pltpu.VMEM((n_tp, ratio, rows, depth), F32),
            pltpu.SemaphoreType.DMA((n_tp,)),
            pltpu.SemaphoreType.DMA((n_tp,)),
            pltpu.VMEM((n_ep, slots, model), BF16),
            pltpu.VMEM((n_ep, slots, model), BF16),
            pltpu.SemaphoreType.DMA((n_ep,)),
            pltpu.SemaphoreType.DMA((n_ep,)),
            pltpu.VMEM((2, half, rows, 2 * hidden), F32),
            pltpu.VMEM((half, rows, 2 * hidden), F32),
            pltpu.SemaphoreType.DMA((1,)),
            pltpu.SemaphoreType.DMA((1,)),
            pltpu.VMEM((half, rows, 2 * hidden), BF16),
            pltpu.VMEM((half, rows, 2 * hidden), BF16),
            pltpu.SemaphoreType.DMA((half,)),
            pltpu.SemaphoreType.DMA((half,)),
            pltpu.VMEM((n_tp, n_ep * slots, chunk), BF16),
            pltpu.VMEM((n_tp, n_ep * slots, chunk), BF16),
            pltpu.SemaphoreType.DMA((n_tp,)),
            pltpu.SemaphoreType.DMA((n_tp,)),
            pltpu.VMEM((n_ep, slots, chunk), BF16),
            pltpu.VMEM((n_ep, slots, chunk), BF16),
            pltpu.SemaphoreType.DMA((n_ep,)),
            pltpu.SemaphoreType.DMA((n_ep,)),
            pltpu.VMEM((rows, hidden), BF16),
            pltpu.VMEM((n_ep, rows, hidden), BF16),
            pltpu.SemaphoreType.DMA((n_ep,)),
            pltpu.SemaphoreType.DMA((n_ep,)),
            pltpu.VMEM((n_tp, group_rows, depth), BF16),
            pltpu.VMEM((n_tp, group_rows, depth), BF16),
            pltpu.SemaphoreType.DMA((n_tp,)),
            pltpu.SemaphoreType.DMA((n_tp,)),
            pltpu.VMEM((ratio, rows, depth), BF16),
            pltpu.VMEM((n_ep, rows, depth), BF16),
            pltpu.SemaphoreType.DMA((n_ep,)),
            pltpu.SemaphoreType.DMA((n_ep,)),
            pltpu.VMEM((rows, chunk), F32),
            pltpu.VMEM((n_tp, rows, chunk), F32),
            pltpu.SemaphoreType.DMA((n_tp,)),
            pltpu.SemaphoreType.DMA((n_tp,)),
        ],
        compiler_params=pltpu.CompilerParams(
            collective_id=0, has_side_effects=True, vmem_limit_bytes=60 * 1024 * 1024
        ),
    )(*scalars, *small, *large)


def shards(
    tokens,
    attn_gain,
    query_weight,
    key_weight,
    value_weight,
    forget_weight,
    forget_bias,
    cache_keys,
    cache_values,
    cache_gates,
    lengths,
    output_weight,
    ffn_gain,
    dense_gate_proj,
    dense_up_proj,
    dense_down_proj,
    dense_mix,
    expert_ids,
    group_prob,
    pair_prob,
    expert_gate,
    expert_up,
    expert_down,
):
    seq_count = tokens.shape[0]
    n_ep = lax.axis_size("ep")
    n_tp = lax.axis_size("tp")
    expert_count = n_ep * expert_gate.shape[0]
    capacity = max(4 * seq_count // expert_count, 8)
    slot_total = expert_count * capacity
    picks = expert_ids.reshape(-1)
    same = (picks[:, None] == picks[None, :]).astype(jnp.int32)
    before = jnp.tril(jnp.ones((2 * seq_count, 2 * seq_count), jnp.int32), -1)
    slot_rank = jnp.sum(same * before, axis=1)
    destination = (picks * capacity + slot_rank).reshape(seq_count, 2)
    slot_grid = jnp.arange(slot_total, dtype=jnp.int32)
    select_first = (destination[:, 0:1] == slot_grid[None, :]).astype(jnp.bfloat16)
    select_second = (destination[:, 1:2] == slot_grid[None, :]).astype(jnp.bfloat16)
    to_slots = (select_first + select_second).T
    routes = group_prob[:, None] * pair_prob / jnp.sum(pair_prob, axis=1, keepdims=True)
    model = (1, tokens.shape[1])
    return layer(
        n_ep,
        n_tp,
        capacity,
        (forget_bias.reshape(1, -1), lengths.reshape(1, -1)),
        (
            tokens,
            attn_gain.reshape(model),
            forget_weight.T,
            cache_gates,
            ffn_gain.reshape(model),
            ffn_gain.reshape(n_ep, 1, -1),
            dense_mix.reshape(model),
            to_slots,
            select_first,
            select_second,
            routes,
        ),
        (
            query_weight,
            key_weight,
            value_weight,
            cache_keys,
            cache_values,
            output_weight,
            dense_gate_proj,
            dense_up_proj,
            expert_gate,
            expert_up,
            expert_down,
            dense_down_proj,
        ),
    )


def solution(mesh):
    return jax.shard_map(
        shards,
        mesh=mesh,
        in_specs=(
            P("ep", None),
            P(),
            P("ep", "tp"),
            P("ep", "tp"),
            P("ep", "tp"),
            P(None, "tp"),
            P("tp"),
            P("ep", "tp", None, None),
            P("ep", "tp", None, None),
            P("ep", "tp", None),
            P("ep"),
            P("tp", "ep"),
            P(),
            P("ep", "tp"),
            P("ep", "tp"),
            P("tp", "ep"),
            P(),
            P("ep", None),
            P("ep"),
            P("ep", None),
            P("ep", None, "tp"),
            P("ep", None, "tp"),
            P("ep", "tp", None),
        ),
        out_specs=P("ep", None),
        check_vma=False,
    )
```
